512 devices in a mesh: grp: 2 (over y), sp: 32 (over z), tp: 8 (over x, core).
Axes of the slice: x: 4, y: 2, z: 32, core: 2. Of those that a mesh axis runs over, the one named last changes fastest.
The devices are a block of a 4x8x32 slice.
Arguments:
- tokens: bfloat16 [16384, 4096], P(('grp', 'sp', 'tp')), parts along dimension 0, may hold values from -8 to 8
- input_gain: float32 [4096], replicated, may hold values from 0.1 to 1.9
- w_query: bfloat16 [4096, 2048], P('sp', 'tp'), may hold values from -0.09375 to 0.09375
- w_key: bfloat16 [4096, 512], P('sp'), may hold values from -0.09375 to 0.09375
- w_value: bfloat16 [4096, 512], P('sp'), may hold values from -0.09375 to 0.09375
- query_gain: float32 [128], replicated, may hold values from 0.1 to 17
- key_gain: float32 [128], replicated, may hold values from 0.1 to 15
- w_out: bfloat16 [2048, 4096], P('tp', 'sp'), may hold values from -0.5 to 0.5
Outputs:
- mixed: bfloat16 [16384, 4096], P(('grp', 'sp', 'tp')), parts along dimension 0
The draws below stay inside these ranges and needn't reach their ends.
There are 2 independent parts, one for each index of `grp`. The reference program is written for one: setup_inputs(seed, part) draws one part's arguments, and reference() takes and returns one part's arrays. A program takes and returns all parts, laid end to end along the dimension named above; an argument that names none is the same for every part. Nothing has to cross between parts.
All inputs are finite; a program needn't handle non-finite values.
Results may differ from the reference program's by a relative error of at most 0.02.
The reference program's roundings to bfloat16 on the way count: a program that leaves them out, or rounds other values in their place, can miss the bound.
Values may be sent and summed in bfloat16 or wider, within the bound.
A program may use at most 64 MiB of HBM per device.

```python
import jax
import jax.numpy as jnp
from jax import lax

D = 4096
HEADS = 16
KV_HEADS = 4
HEAD = 128
GRID_W = 64
TOK_DEV = 256
TOKENS = 8192
N_TP = 8


def draw_tokens(key, part):
    first, second = jax.random.split(jax.random.fold_in(key, 11))
    spread_part = jax.random.normal(first, (TOKENS, D), jnp.float32)
    shifts = jax.random.normal(second, (TOKENS // TOK_DEV, D), jnp.float32) * 0.8
    return jnp.clip(spread_part + jnp.repeat(shifts, TOK_DEV, axis=0), -8.0, 8.0).astype(jnp.bfloat16)


def draw_query_gain(key, part):
    inner = jax.random.fold_in(key, 23)
    return jnp.clip(1.0 + 0.18 * jax.random.normal(inner, (HEAD,), jnp.float32), 0.1, 1.9)


def draw_key_gain(key, part):
    inner = jax.random.fold_in(key, 37)
    return jnp.clip(1.0 + 0.18 * jax.random.normal(inner, (HEAD,), jnp.float32), 0.1, 1.9)


def shard_levels(key, extent, pieces, least, high):
    def one(position, parts):
        heights = jax.random.uniform(jax.random.fold_in(jax.random.fold_in(key, 6), position), (parts,), jnp.float32, least / len(pieces), high / len(pieces))
        return jnp.repeat(jnp.exp(heights), extent[position] // parts).reshape((-1,) + (1,) * (len(extent) - position - 1))

    factor_of = one(*pieces[0])
    for cut in pieces[1:]:
        factor_of = factor_of * one(*cut)
    return factor_of


def bell_draw(rng, dims, scale, limit, pieces=(), kind=jnp.bfloat16):
    values = jax.random.normal(rng, dims, jnp.float32) * scale
    if len(pieces) > 0:
        values = shard_levels(rng, dims, pieces, -0.22, 0.18) * values
    return jnp.clip(values, min=-limit, max=limit).astype(kind)


def setup_inputs(seed: int = 0, part: int = 0) -> dict:
    arg_keys = jax.random.split(jax.random.key(seed), 9)
    own_keys = jax.random.split(jax.random.fold_in(arg_keys[8], part), 9)
    tokens = draw_tokens(jax.random.fold_in(jax.random.fold_in(arg_keys[8], part), 71), part)
    input_gain = jnp.clip(1.0 + 0.18 * jax.random.normal(arg_keys[1], (D,), jnp.float32), 0.1, 1.9)
    w_query = bell_draw(arg_keys[2], (D, HEADS * HEAD), D ** -0.5, 0.09375, ((0, 32), (1, 8)))
    w_key = bell_draw(arg_keys[3], (D, KV_HEADS * HEAD), D ** -0.5, 0.09375, ((0, 32),))
    w_value = bell_draw(arg_keys[4], (D, KV_HEADS * HEAD), D ** -0.5, 0.09375, ((0, 32),))
    query_gain = draw_query_gain(jax.random.fold_in(arg_keys[8], 71), part)
    key_gain = draw_key_gain(jax.random.fold_in(arg_keys[8], 71), part)
    w_out = bell_draw(arg_keys[7], (HEADS * HEAD, D), (HEADS * HEAD // 16) ** -0.5, 0.5, ((0, 8), (1, 32)))
    return {"tokens": tokens, "input_gain": input_gain, "w_query": w_query, "w_key": w_key, "w_value": w_value, "query_gain": query_gain, "key_gain": key_gain, "w_out": w_out}


eps = 1e-06

def rms_rows(values, gain):
    floats = values.astype(jnp.float32)
    scale = lax.rsqrt(lax.optimization_barrier(jnp.mean(floats * floats, axis=-1, keepdims=True)) + eps)
    return floats * scale * gain

def rotate_half(part, angles):
    first, second = jnp.split(part, 2, axis=-1)
    cosine = jnp.cos(angles)
    sine = jnp.sin(angles)
    return jnp.concatenate([first * cosine - second * sine, second * cosine + first * sine], axis=-1)

def turn_heads(heads, gain, positions):
    normed = rms_rows(heads, gain)
    quarter = heads.shape[-1] // 4
    inverse = 10000.0 ** (-jnp.arange(quarter, dtype=jnp.float32) * 2.0 / (2 * quarter))
    grid_row = (positions // GRID_W).astype(jnp.float32)
    grid_col = (positions % GRID_W).astype(jnp.float32)
    row_angle = (grid_row[:, None] * inverse[None, :])[:, None, :]
    col_angle = (grid_col[:, None] * inverse[None, :])[:, None, :]
    row_part, col_part = jnp.split(normed, 2, axis=-1)
    return jnp.concatenate([rotate_half(row_part, row_angle), rotate_half(col_part, col_angle)], axis=-1)

def reference(tokens, input_gain, w_query, w_key, w_value, query_gain, key_gain, w_out):
    count = tokens.shape[0]
    normed = rms_rows(tokens, input_gain).astype(jnp.bfloat16)
    query = jnp.dot(normed, w_query, preferred_element_type=jnp.float32).astype(jnp.bfloat16)
    key = jnp.dot(normed, w_key, preferred_element_type=jnp.float32).astype(jnp.bfloat16)
    value = jnp.dot(normed, w_value, preferred_element_type=jnp.float32).astype(jnp.bfloat16)
    positions = jnp.arange(count, dtype=jnp.int32)
    turned_query = (turn_heads(query.reshape(count, HEADS, HEAD), query_gain, positions) * HEAD ** (-0.5)).astype(jnp.bfloat16)
    turned_key = turn_heads(key.reshape(count, KV_HEADS, HEAD), key_gain, positions).astype(jnp.bfloat16)
    value_heads = value.reshape(count, KV_HEADS, HEAD)
    block = min(512, count)
    group = HEADS // KV_HEADS
    outputs = []
    for head in range(HEADS):
        keys = turned_key[:, head // group, :]
        values = value_heads[:, head // group, :]
        queries = turned_query[:, head, :].reshape(count // block, block, HEAD)

        def attend(rows):
            scores = lax.dot_general(rows, keys, (((1,), (1,)), ((), ())), preferred_element_type=jnp.float32)
            peak = lax.optimization_barrier(jnp.max(scores, axis=1, keepdims=True))
            weights = jnp.exp(scores - peak)
            total = lax.optimization_barrier(jnp.sum(weights, axis=1, keepdims=True))
            summed = jnp.dot(weights.astype(jnp.bfloat16), values, preferred_element_type=jnp.float32)
            return (summed / total).astype(jnp.bfloat16)
        outputs.append(lax.map(attend, queries).reshape(count, HEAD))
    attended = jnp.concatenate(outputs, axis=1)
    width = HEADS * HEAD // N_TP
    mixed = jnp.zeros((count, tokens.shape[1]), jnp.float32)
    for index in range(N_TP):
        term = jnp.dot(attended[:, index * width:(index + 1) * width], w_out[index * width:(index + 1) * width, :], preferred_element_type=jnp.float32)
        mixed = mixed + term.astype(jnp.bfloat16).astype(jnp.float32)
    return mixed.astype(jnp.bfloat16)
```

```python
import functools

import jax
import jax.numpy as jnp
from jax import lax
from jax.experimental import pallas as pl
from jax.experimental.pallas import tpu as pltpu
from jax.sharding import PartitionSpec as P

HEAD = 128
GRID_W = 64
EPS = 1e-06
CHUNKS = 2
QUARTERS = 4
MESH = pl.DeviceIdType.MESH


def remote(src, dst, send_sem, recv_sem, device):
    return pltpu.make_async_remote_copy(
        src_ref=src, dst_ref=dst, send_sem=send_sem, recv_sem=recv_sem, device_id=device, device_id_type=MESH
    )


def fused(
    sizes,
    tok_hbm,
    gain_ref,
    wq_hbm,
    wk_hbm,
    wv_hbm,
    qg_ref,
    kg_ref,
    wo_hbm,
    inv_ref,
    out_ref,
    tok,
    normed,
    wa,
    wo,
    kv,
    cosine,
    sine,
    queries,
    peak,
    total,
    summed,
    terms,
    partner_terms,
    pair_sums,
    arrived,
    in_sems,
    nx_ss,
    nx_rs,
    nd_ss,
    nd_rs,
    wa_ss,
    wa_rs,
    wy_ss,
    wy_rs,
    kv_ss,
    kv_rs,
    kd_ss,
    kd_rs,
    wo_ss,
    wo_rs,
    td_ss,
    td_rs,
    x_ss,
    x_rs,
):
    n, n_tp = sizes
    chips = n_tp // 2
    hops = n // 2
    grp, z, t = lax.axis_index("grp"), lax.axis_index("sp"), lax.axis_index("tp")
    x, core = t // 2, t % 2
    half = grp % 2
    right, left = {"sp": lax.rem(z + 1, n)}, {"sp": lax.rem(z + n - 1, n)}
    mate = {"tp": t + 1 - 2 * core}
    twin = {"grp": grp + 1 - 2 * half}
    across = [{"tp": lax.rem(t + 2 * d, n_tp)} for d in range(1, chips)]

    own_rows, width = tok.shape
    rows = own_rows * n_tp
    depth = wa.shape[1]
    q_cols = wa.shape[2] - HEAD
    heads = q_cols // HEAD
    half_depth = depth // 2
    out_rows = wo.shape[1]
    half_out = out_rows // 2

    loads = [
        pltpu.make_async_copy(wq_hbm, wa.at[z, :, pl.ds(0, q_cols)], in_sems.at[0]),
        pltpu.make_async_copy(wo_hbm, wo.at[z], in_sems.at[2]),
        pltpu.make_async_copy(tok_hbm, tok, in_sems.at[3]),
    ]
    for load in loads:
        load.start()
    columns = pl.ds(pl.multiple_of(x * HEAD, HEAD), HEAD)

    @pl.when(core == 0)
    def _():
        pltpu.make_async_copy(wk_hbm.at[:, columns], wa.at[z, :, pl.ds(q_cols, HEAD)], in_sems.at[1]).start()

    @pl.when(core == 1)
    def _():
        pltpu.make_async_copy(wv_hbm.at[:, columns], wa.at[z, :, pl.ds(q_cols, HEAD)], in_sems.at[1]).start()

    barrier = pltpu.get_barrier_semaphore()
    peers = [right, left, mate, twin] + across
    for peer in peers:
        pl.semaphore_signal(barrier, inc=1, device_id=peer, device_id_type=MESH)
    pl.semaphore_wait(barrier, len(peers))

    def back(s):
        return lax.rem(z - s + n, n)

    def ahead(s):
        return lax.rem(z + s, n)

    piece_rows = half_depth // CHUNKS

    def wa_ring(way, slot, s, c):
        first = pl.multiple_of(half * half_depth + c * piece_rows, piece_rows)
        piece = wa.at[slot, pl.ds(first, piece_rows), :]
        return remote(piece, piece, wa_ss.at[way], wa_rs.at[way, s, c], right if way == 0 else left)

    def wa_twin(slot):
        piece = wa.at[slot, pl.ds(pl.multiple_of(half * half_depth, half_depth), half_depth), :]
        return remote(piece, piece, wy_ss.at[0], wy_rs.at[0], twin)

    def wo_ring(way, slot, s):
        piece = wo.at[slot, pl.ds(pl.multiple_of(half * half_out, half_out), half_out), :]
        return remote(piece, piece, wo_ss.at[way], wo_rs.at[way, s], right if way == 0 else left)

    def wo_twin(slot):
        piece = wo.at[slot, pl.ds(pl.multiple_of(half * half_out, half_out), half_out), :]
        return remote(piece, piece, wy_ss.at[1], wy_rs.at[1], twin)

    def kv_ring(way, slot, s, c):
        piece = kv.at[core, slot, pl.ds(c * (rows // CHUNKS), rows // CHUNKS), :]
        return remote(piece, piece, kv_ss.at[way], kv_rs.at[way, s, c], right if way == 0 else left)

    def kv_mate(way, slot, s, c):
        piece = kv.at[core, slot, pl.ds(c * (rows // CHUNKS), rows // CHUNKS), :]
        return remote(piece, piece, kd_ss.at[0], kd_rs.at[way, s], mate)

    def kv_from_mate(way, slot, s):
        block = kv.at[1 - core, slot]
        return remote(block, block, kd_ss.at[0], kd_rs.at[way, s], mate)

    loads[0].wait()
    pltpu.make_async_copy(wk_hbm.at[:, columns], wa.at[z, :, pl.ds(q_cols, HEAD)], in_sems.at[1]).wait()
    for c in range(CHUNKS):
        wa_ring(0, z, 0, c).start()
        wa_ring(1, z, 0, c).start()

    loads[2].wait()
    floats = tok[...].astype(jnp.float32)
    scale = lax.rsqrt(jnp.mean(floats * floats, axis=-1, keepdims=True) + EPS)
    normed[t] = (floats * scale * gain_ref[...]).astype(jnp.bfloat16)

    def normed_to(d):
        return remote(normed.at[t], normed.at[t], nx_ss.at[d - 1], nx_rs.at[d - 1], across[d - 1])

    def normed_mate(d):
        slot = lax.rem(t + n_tp - 2 * d, n_tp)
        return remote(normed.at[slot], normed.at[slot], nd_ss.at[d], nd_rs.at[d], mate)

    def normed_from(d):
        slot = lax.rem(t + n_tp - 2 * d, n_tp)
        return remote(normed.at[slot], normed.at[slot], nx_ss.at[d - 1], nx_rs.at[d - 1], across[d - 1])

    def normed_from_mate(d):
        slot = lax.rem(t + 1 - 2 * core + n_tp - 2 * d, n_tp)
        return remote(normed.at[slot], normed.at[slot], nd_ss.at[d], nd_rs.at[d], mate)

    for d in range(1, chips):
        normed_to(d).start()
    normed_mate(0).start()

    lane = lax.broadcasted_iota(jnp.int32, (rows, HEAD), 1)
    place = lax.broadcasted_iota(jnp.int32, (rows, HEAD), 0) + z * rows
    spot = jnp.where(lane < HEAD // 2, place // GRID_W, place % GRID_W).astype(jnp.float32)
    angles = spot * inv_ref[...]
    first_half = lane % (HEAD // 2) < HEAD // 4
    cosine[...] = jnp.cos(angles)
    sine[...] = jnp.where(first_half, -jnp.sin(angles), jnp.sin(angles))

    def turned(raw, gain):
        heads_in = raw.astype(jnp.bfloat16).astype(jnp.float32)
        scale = lax.rsqrt(jnp.mean(heads_in * heads_in, axis=-1, keepdims=True) + EPS)
        scaled = heads_in * scale * gain
        lanes = lax.broadcasted_iota(jnp.int32, scaled.shape, 1)
        other = jnp.where(
            lanes % (HEAD // 2) < HEAD // 4,
            pltpu.roll(scaled, HEAD - HEAD // 4, 1),
            pltpu.roll(scaled, HEAD // 4, 1),
        )
        return scaled * cosine[...] + other * sine[...]

    def wa_step(s, carry):
        for c in range(CHUNKS):
            wa_ring(0, back(s), s - 1, c).wait_recv()
            wa_ring(0, back(s), s, c).start()
            wa_ring(1, ahead(s), s - 1, c).wait_recv()

            @pl.when(s < hops - 1)
            def _():
                wa_ring(1, ahead(s), s, c).start()

        wa_twin(back(s)).start()
        wa_twin(ahead(s)).start()
        return carry

    split = hops - 4
    lax.fori_loop(1, split, wa_step, 0)
    for d in range(1, chips):
        normed_from(d).wait_recv()
        normed_mate(d).start()
    lax.fori_loop(split, hops, wa_step, 0)
    for c in range(CHUNKS):
        wa_ring(0, back(hops), hops - 1, c).wait_recv()
    wa_twin(back(hops)).start()
    for d in range(chips):
        normed_from_mate(d).wait_recv()
    incoming = wa.at[pl.ds(0, n - 1), pl.ds(0, half_depth), :]
    remote(incoming, incoming, wy_ss.at[0], wy_rs.at[0], twin).wait_recv()

    tokens_in = normed[...].reshape(rows, width)
    projected = jnp.dot(
        tokens_in, wa[:, :, q_cols:].reshape(width, HEAD), preferred_element_type=jnp.float32
    )

    @pl.when(core == 0)
    def _():
        kv[0, z] = turned(projected, kg_ref[...]).astype(jnp.bfloat16)

    @pl.when(core == 1)
    def _():
        kv[1, z] = projected.astype(jnp.bfloat16)

    loads[1].wait()
    for c in range(CHUNKS):
        kv_ring(0, z, 0, c).start()
        kv_ring(1, z, 0, c).start()
    for c in range(CHUNKS):
        kv_mate(0, z, 0, c).start()
    wo_ring(0, z, 0).start()
    wo_ring(1, z, 0).start()

    for h in range(heads):
        raw = jnp.dot(
            normed[...].reshape(rows, width),
            wa[:, :, h * HEAD : (h + 1) * HEAD].reshape(width, HEAD),
            preferred_element_type=jnp.float32,
        )
        queries[h] = (turned(raw, qg_ref[...]) * HEAD ** (-0.5)).astype(jnp.bfloat16)

    peak[...] = jnp.full_like(peak, -1e30)
    total[...] = jnp.zeros_like(total)
    summed[...] = jnp.zeros_like(summed)

    def attend(a, b):
        for h in range(heads):
            q = queries[h]
            scores = [
                lax.dot_general(q, kv[0, i], (((1,), (1,)), ((), ())), preferred_element_type=jnp.float32)
                for i in (a, b)
            ]
            old = peak[h]
            new = jnp.maximum(old, jnp.max(jnp.maximum(*scores), axis=1, keepdims=True))
            fade = jnp.exp(old - new)
            wide = jnp.concatenate([new] * (rows // HEAD), axis=1)
            weights = [jnp.exp(part - wide) for part in scores]
            peak[h] = new
            total[h] = fade * total[h] + jnp.sum(weights[0] + weights[1], axis=1, keepdims=True)
            summed[h] = (
                fade * summed[h]
                + jnp.dot(weights[0].astype(jnp.bfloat16), kv[1, a], preferred_element_type=jnp.float32)
                + jnp.dot(weights[1].astype(jnp.bfloat16), kv[1, b], preferred_element_type=jnp.float32)
            )

    def kv_step(s, carry):
        for c in range(CHUNKS):
            kv_ring(0, back(s), s - 1, c).wait_recv()
            kv_ring(0, back(s), s, c).start()
            kv_mate(0, back(s), s, c).start()
            kv_ring(1, ahead(s), s - 1, c).wait_recv()

            @pl.when(s < hops - 1)
            def _():
                kv_ring(1, ahead(s), s, c).start()

            kv_mate(1, ahead(s), s, c).start()
        wo_ring(0, back(s), s - 1).wait_recv()
        wo_ring(0, back(s), s).start()
        wo_twin(back(s)).start()
        wo_ring(1, ahead(s), s - 1).wait_recv()

        @pl.when(s < hops - 1)
        def _():
            wo_ring(1, ahead(s), s).start()

        wo_twin(ahead(s)).start()

        @pl.when(s > 1)
        def _():
            kv_from_mate(0, back(s - 1), s - 1).wait_recv()
            kv_from_mate(1, ahead(s - 1), s - 1).wait_recv()
            attend(back(s - 1), ahead(s - 1))

        return carry

    lax.fori_loop(1, hops, kv_step, 0)
    for c in range(CHUNKS):
        kv_ring(0, back(hops), hops - 1, c).wait_recv()
        kv_mate(0, back(hops), hops, c).start()
    wo_ring(0, back(hops), hops - 1).wait_recv()
    wo_twin(back(hops)).start()
    kv_from_mate(0, back(hops - 1), hops - 1).wait_recv()
    kv_from_mate(1, ahead(hops - 1), hops - 1).wait_recv()
    attend(back(hops - 1), ahead(hops - 1))
    kv_from_mate(0, z, 0).wait_recv()
    kv_from_mate(0, back(hops), hops).wait_recv()
    attend(z, back(hops))

    attended = jnp.concatenate([(summed[h] / total[h]).astype(jnp.bfloat16) for h in range(heads)], axis=1)

    incoming = wo.at[pl.ds(0, n - 1), pl.ds(0, half_out), :]
    remote(incoming, incoming, wy_ss.at[1], wy_rs.at[1], twin).wait_recv()

    per_piece = n // QUARTERS
    cols = wo.shape[2]

    def term_mate(p):
        return remote(terms.at[p, 1 - core], partner_terms.at[p], td_ss.at[p], td_rs.at[p], mate)

    def project(p, carry):
        for j in range(per_piece // 2):
            both = jnp.concatenate([wo[p * per_piece + 2 * j], wo[p * per_piece + 2 * j + 1]], axis=1)
            term = jnp.dot(attended, both, preferred_element_type=jnp.float32).astype(jnp.bfloat16)
            for owner in range(n_tp):
                terms[p, owner % 2, owner // 2, :, 2 * j * cols : (2 * j + 2) * cols] = term[
                    owner * own_rows : (owner + 1) * own_rows
                ]
        term_mate(p).start()
        return carry

    lax.fori_loop(0, QUARTERS, project, 0)

    def sum_to(p, d):
        there = lax.rem(x + d, chips)
        return remote(
            pair_sums.at[p, there], arrived.at[p, d - 1], x_ss.at[p, d - 1], x_rs.at[p, d - 1], across[d - 1]
        )

    far_first = sorted(range(1, chips), key=lambda d: -min(d, chips - d))

    def exchange(p, carry):
        term_mate(p).wait_recv()
        pair_sums[p] = (
            terms[p, core].astype(jnp.float32) + partner_terms[p].astype(jnp.float32)
        ).astype(jnp.bfloat16)
        for d in far_first:
            sum_to(p, d).start()
        return carry

    lax.fori_loop(0, QUARTERS, exchange, 0)
    piece_cols = per_piece * cols
    for p in range(QUARTERS):
        mixed = terms[p, core, x].astype(jnp.float32) + partner_terms[p, x].astype(jnp.float32)
        for d in range(1, chips):
            sum_to(p, d).wait_recv()
            mixed = mixed + arrived[p, d - 1].astype(jnp.float32)
        out_ref[:, p * piece_cols : (p + 1) * piece_cols] = mixed.astype(out_ref.dtype)

    for d in range(1, chips):
        normed_to(d).wait_send()
    for d in range(chips):
        normed_mate(d).wait_send()
    for way, count in ((0, hops), (1, hops - 1)):
        sent = wa.at[pl.ds(0, count), pl.ds(0, half_depth), :]
        remote(sent, sent, wa_ss.at[way], wa_rs.at[way, 0, 0], right).wait_send()
        sent = wo.at[pl.ds(0, count), pl.ds(0, half_out), :]
        remote(sent, sent, wo_ss.at[way], wo_rs.at[way, 0], right).wait_send()
        sent = kv.at[0, pl.ds(0, count)]
        remote(sent, sent, kv_ss.at[way], kv_rs.at[way, 0, 0], right).wait_send()
    sent = wa.at[pl.ds(0, n - 1), pl.ds(0, half_depth), :]
    remote(sent, sent, wy_ss.at[0], wy_rs.at[0], twin).wait_send()
    sent = wo.at[pl.ds(0, n - 1), pl.ds(0, half_out), :]
    remote(sent, sent, wy_ss.at[1], wy_rs.at[1], twin).wait_send()
    remote(kv.at[0], kv.at[0], kd_ss.at[0], kd_rs.at[0, 0], mate).wait_send()
    for p in range(QUARTERS):
        term_mate(p).wait_send()
        for d in range(1, chips):
            sum_to(p, d).wait_send()


def solution(mesh):
    n, n_tp = mesh.shape["sp"], mesh.shape["tp"]

    def local(tokens, input_gain, w_query, w_key, w_value, query_gain, key_gain, w_out):
        own_rows, width = tokens.shape
        rows = own_rows * n_tp
        depth, q_cols = w_query.shape
        heads = q_cols // HEAD
        out_rows, cols = w_out.shape
        chips = n_tp // 2
        hops = n // 2
        piece_cols = width // QUARTERS
        quarter = HEAD // 4
        inverse = 10000.0 ** (-jnp.arange(quarter, dtype=jnp.float32) * 2.0 / (2 * quarter))
        inverse = jnp.tile(inverse, 4)[None, :]
        bf16, f32 = jnp.bfloat16, jnp.float32
        dma = pltpu.SemaphoreType.DMA
        any_spec = pl.BlockSpec(memory_space=pl.ANY)
        vmem_spec = pl.BlockSpec(memory_space=pltpu.VMEM)
        return pl.pallas_call(
            functools.partial(fused, (n, n_tp)),
            out_shape=jax.ShapeDtypeStruct((own_rows, width), bf16),
            in_specs=[
                any_spec,
                vmem_spec,
                any_spec,
                any_spec,
                any_spec,
                vmem_spec,
                vmem_spec,
                any_spec,
                vmem_spec,
            ],
            out_specs=vmem_spec,
            scratch_shapes=[
                pltpu.VMEM((own_rows, width), bf16),
                pltpu.VMEM((n_tp, own_rows, width), bf16),
                pltpu.VMEM((n, depth, q_cols + HEAD), bf16),
                pltpu.VMEM((n, out_rows, cols), bf16),
                pltpu.VMEM((2, n, rows, HEAD), bf16),
                pltpu.VMEM((rows, HEAD), f32),
                pltpu.VMEM((rows, HEAD), f32),
                pltpu.VMEM((heads, rows, HEAD), bf16),
                pltpu.VMEM((heads, rows, HEAD), f32),
                pltpu.VMEM((heads, rows, HEAD), f32),
                pltpu.VMEM((heads, rows, HEAD), f32),
                pltpu.VMEM((QUARTERS, 2, chips, own_rows, piece_cols), bf16),
                pltpu.VMEM((QUARTERS, chips, own_rows, piece_cols), bf16),
                pltpu.VMEM((QUARTERS, chips, own_rows, piece_cols), bf16),
                pltpu.VMEM((QUARTERS, chips - 1, own_rows, piece_cols), bf16),
                dma((4,)),
                dma((chips - 1,)),
                dma((chips - 1,)),
                dma((chips,)),
                dma((chips,)),
                dma((2,)),
                dma((2, hops, CHUNKS)),
                dma((2,)),
                dma((2,)),
                dma((2,)),
                dma((2, hops, CHUNKS)),
                dma((1,)),
                dma((2, hops + 1)),
                dma((2,)),
                dma((2, hops)),
                dma((QUARTERS,)),
                dma((QUARTERS,)),
                dma((QUARTERS, chips - 1)),
                dma((QUARTERS, chips - 1)),
            ],
            compiler_params=pltpu.CompilerParams(
                collective_id=0, has_side_effects=True, vmem_limit_bytes=48 * 1024 * 1024
            ),
        )(
            tokens,
            input_gain[None, :],
            w_query,
            w_key,
            w_value,
            query_gain[None, :],
            key_gain[None, :],
            w_out,
            inverse,
        )

    in_specs = (
        P(("grp", "sp", "tp"), None),
        P(),
        P("sp", "tp"),
        P("sp", None),
        P("sp", None),
        P(),
        P(),
        P("tp", "sp"),
    )
    out_specs = P(("grp", "sp", "tp"), None)
    return jax.shard_map(local, mesh=mesh, in_specs=in_specs, out_specs=out_specs, check_vma=False)
```

```python
import functools

import jax
import jax.numpy as jnp
import numpy as np
from jax import lax
from jax.experimental import pallas as pl
from jax.experimental.pallas import tpu as pltpu
from jax.sharding import PartitionSpec as P

HEAD = 128
GRID_W = 64
EPS = 1e-06
CHUNKS = 4
FAR = 4
MID = 2
LEAD = 6
QUARTERS = 4
MESH = pl.DeviceIdType.MESH


def remote(src, dst, send_sem, recv_sem, device):
    return pltpu.make_async_remote_copy(
        src_ref=src, dst_ref=dst, send_sem=send_sem, recv_sem=recv_sem, device_id=device, device_id_type=MESH
    )


def fused(
    sizes,
    tok_hbm,
    gain_hbm,
    wq_hbm,
    wk_hbm,
    wv_hbm,
    qg_hbm,
    kg_hbm,
    wo_hbm,
    inv_hbm,
    out_hbm,
    mixed,
    tok,
    gain,
    qg,
    kg,
    inv,
    normed,
    wkv,
    wq,
    wo,
    kv,
    cosine,
    sine,
    queries,
    peak,
    total,
    summed,
    terms,
    partner_terms,
    pair_sums,
    relayed,
    arrived,
    in_sems,
    out_sems,
    nx_ss,
    nx_rs,
    nd_ss,
    nd_rs,
    wkv_ss,
    wkv_rs,
    w_ss,
    w_rs,
    twin_ss,
    twin_rs,
    md_ss,
    md_rs,
    kv_ss,
    kv_rs,
    kd_ss,
    kd_rs,
    td_ss,
    td_rs,
    x_ss,
    x_rs,
):
    n, n_tp = sizes
    chips = n_tp // 2
    hops = n // 2
    grp, z, t = lax.axis_index("grp"), lax.axis_index("sp"), lax.axis_index("tp")
    x, core = t // 2, t % 2
    half = grp % 2
    other_t = t + 1 - 2 * core
    low_t = t - core
    mate = {"tp": other_t}
    other_grp = grp + 1 - 2 * half
    across = [{"tp": lax.rem(t + 2 * d, n_tp)} for d in range(1, chips)]

    own_rows, width = tok.shape
    rows = own_rows * n_tp
    q_cols = wq.shape[3]
    heads = q_cols // HEAD
    cols = wo.shape[3]

    def back(s):
        return lax.rem(z - s + n, n)

    def ahead(s):
        return lax.rem(z + s, n)

    def toward(way, j):
        return ahead(j) if way == 0 else back(j)

    def source(way, d):
        return back(d) if way == 0 else ahead(d)

    columns = pl.ds(pl.multiple_of(x * HEAD, HEAD), HEAD)
    loads = [
        pltpu.make_async_copy(source_ref, target, in_sems.at[i])
        for i, (source_ref, target) in enumerate(
            (
                (wk_hbm.at[:, columns], wkv.at[z, :, pl.ds(0, HEAD)]),
                (wv_hbm.at[:, columns], wkv.at[z, :, pl.ds(HEAD, HEAD)]),
                (tok_hbm, tok),
                (gain_hbm, gain),
                (wq_hbm, wq.at[z, core]),
                (wo_hbm, wo.at[z, core]),
                (qg_hbm, qg),
                (kg_hbm, kg),
                (inv_hbm, inv),
            )
        )
    ]
    for load in loads:
        load.start()

    peers = [mate, {"grp": other_grp}, {"grp": other_grp, "tp": other_t}] + across
    peers += [{"sp": toward(way, j)} for way in (0, 1) for j in range(1, FAR + 1)]
    peers += [{"sp": toward(way, j), "tp": other_t} for way in (0, 1) for j in range(1, MID + 1)]
    barrier = pltpu.get_barrier_semaphore()
    for peer in peers:
        pl.semaphore_signal(barrier, inc=1, device_id=peer, device_id_type=MESH)
    pl.semaphore_wait(barrier, len(peers))

    wkv_half = wkv.shape[1] // 2

    def wkv_piece(slot):
        return wkv.at[slot, pl.ds(pl.multiple_of(half * wkv_half, wkv_half), wkv_half), :]

    def wkv_ring(way, d, j):
        piece = wkv_piece(source(way, d))
        return remote(piece, piece, wkv_ss.at[way], wkv_rs.at[way, d // FAR, j - 1], {"sp": toward(way, j)})

    def wkv_arrival(way, d):
        piece = wkv_piece(source(way, d))
        return remote(
            piece, piece, wkv_ss.at[way], wkv_rs.at[way, (d - 1) // FAR, (d - 1) % FAR], {"sp": toward(way, 1)}
        )

    def wkv_twin(way, d):
        piece = wkv_piece(source(way, d))
        return remote(piece, piece, twin_ss.at[2], twin_rs.at[2], {"grp": other_grp})

    reach = (hops, hops - 1)

    def wkv_send(way, d):
        for j in [FAR] + list(range(1, FAR)):
            if d + j <= reach[way]:
                wkv_ring(way, d, j).start()

    weights = (wq, wo)

    def half_rows(f):
        size = weights[f].shape[2] // 2
        return pl.ds(pl.multiple_of(half * size, size), size)

    def w_piece(f, slot):
        return weights[f].at[slot, :, half_rows(f), :]

    def w_own(f, way, j):
        piece = weights[f].at[z, core, half_rows(f), :]
        return remote(piece, piece, w_ss.at[f], w_rs.at[f, way, 0, j - 1], {"sp": toward(way, j), "tp": low_t})

    def w_ring(f, way, k, j):
        piece = w_piece(f, source(way, MID * k))
        return remote(piece, piece, w_ss.at[f], w_rs.at[f, way, k, j - 1], {"sp": toward(way, j)})

    def w_arrival(f, way, k, j):
        piece = w_piece(f, source(way, MID * k + j))
        return remote(piece, piece, w_ss.at[f], w_rs.at[f, way, k, j - 1], {"sp": toward(way, 1)})

    def w_share(f, way, d):
        slot = source(way, d)
        for c in (0, 1):
            piece = weights[f].at[slot, c, half_rows(f), :]
            remote(piece, piece, twin_ss.at[f], twin_rs.at[f], {"grp": other_grp, "tp": low_t + c}).start()
        piece = weights[f].at[slot, 1, half_rows(f), :]
        remote(piece, piece, md_ss.at[f], md_rs.at[f], mate).start()

    def several(f, count, c=None):
        size = weights[f].shape[2] // 2
        if c is None:
            return weights[f].at[pl.ds(0, count), :, pl.ds(0, size), :]
        return weights[f].at[pl.ds(0, count), c, pl.ds(0, size), :]

    chunk = 2 * rows // CHUNKS

    def kv_piece(slot, c):
        return kv.at[slot, c * chunk // rows, pl.ds(c * chunk % rows, chunk), :]

    def kv_ring(way, slot, s, c):
        piece = kv_piece(slot, c)
        return remote(piece, piece, kv_ss.at[way], kv_rs.at[way, s, c], {"sp": toward(way, 1)})

    def kv_mate(way, slot, s, c):
        piece = kv_piece(slot, c)
        return remote(piece, piece, kd_ss.at[0], kd_rs.at[way, s], mate)

    def kv_from_mate(way, slot, s):
        return remote(kv.at[slot], kv.at[slot], kd_ss.at[0], kd_rs.at[way, s], mate)

    def normed_to(d):
        return remote(normed.at[t], normed.at[t], nx_ss.at[d - 1], nx_rs.at[d - 1], across[d - 1])

    def normed_slot(d, of):
        return normed.at[lax.rem(of + n_tp - 2 * d, n_tp)]

    def normed_mate(d):
        return remote(normed_slot(d, t), normed_slot(d, t), nd_ss.at[d], nd_rs.at[d], mate)

    def normed_from(d):
        return remote(normed_slot(d, t), normed_slot(d, t), nx_ss.at[d - 1], nx_rs.at[d - 1], across[d - 1])

    def normed_from_mate(d):
        return remote(normed_slot(d, other_t), normed_slot(d, other_t), nd_ss.at[d], nd_rs.at[d], mate)

    loads[0].wait()
    loads[1].wait()

    @pl.when(core == 1)
    def _():
        wkv_send(0, 0)
        wkv_send(1, 0)

    loads[2].wait()
    loads[3].wait()
    floats = tok[...].astype(jnp.float32)
    scale = lax.rsqrt(jnp.mean(floats * floats, axis=-1, keepdims=True) + EPS)
    normed[t] = (floats * scale * gain[...]).astype(jnp.bfloat16)
    for d in range(1, chips):
        normed_to(d).start()
    normed_mate(0).start()

    def w_own_sends(f):
        loads[4 + f].wait()
        for j in range(MID, 0, -1):
            for way in (0, 1):
                w_own(f, way, j).start()

    w_own_sends(0)
    for load in loads[6:]:
        load.wait()

    lane = lax.broadcasted_iota(jnp.int32, (rows, HEAD), 1)
    place = lax.broadcasted_iota(jnp.int32, (rows, HEAD), 0) + z * rows
    spot = jnp.where(lane < HEAD // 2, place // GRID_W, place % GRID_W).astype(jnp.float32)
    angles = spot * inv[...]
    first_half = lane % (HEAD // 2) < HEAD // 4
    cosine[...] = jnp.cos(angles)
    sine[...] = jnp.where(first_half, -jnp.sin(angles), jnp.sin(angles))
    peak[...] = jnp.full_like(peak, -1e30)
    total[...] = jnp.zeros_like(total)
    summed[...] = jnp.zeros_like(summed)

    def turned(raw, head_gain):
        heads_in = raw.astype(jnp.bfloat16).astype(jnp.float32)
        scale = lax.rsqrt(jnp.mean(heads_in * heads_in, axis=-1, keepdims=True) + EPS)
        scaled = heads_in * scale * head_gain
        lanes = lax.broadcasted_iota(jnp.int32, scaled.shape, 1)
        other = jnp.where(
            lanes % (HEAD // 2) < HEAD // 4,
            pltpu.roll(scaled, HEAD - HEAD // 4, 1),
            pltpu.roll(scaled, HEAD // 4, 1),
        )
        return scaled * cosine[...] + other * sine[...]

    def query_weights_here():
        incoming = several(0, n - 1, 0)
        remote(incoming, incoming, twin_ss.at[0], twin_rs.at[0], mate).wait_recv()

    def make_queries(first, count):
        raw = jnp.dot(
            normed[...].reshape(rows, width),
            wq[:, core, :, first * HEAD : (first + count) * HEAD].reshape(width, count * HEAD),
            preferred_element_type=jnp.float32,
        )
        for h in range(count):
            queries[first + h] = (turned(raw[:, h * HEAD : (h + 1) * HEAD], qg[...]) * HEAD ** (-0.5)).astype(
                jnp.bfloat16
            )

    def attend(a, b):
        for h in range(heads):
            q = queries[h]
            scores = [
                lax.dot_general(q, kv[i, 0], (((1,), (1,)), ((), ())), preferred_element_type=jnp.float32)
                for i in (a, b)
            ]
            old = peak[h]
            new = jnp.maximum(old, jnp.max(jnp.maximum(*scores), axis=1, keepdims=True))
            fade = jnp.exp(old - new)
            wide = jnp.concatenate([new] * (rows // HEAD), axis=1)
            parts = [jnp.exp(part - wide) for part in scores]
            peak[h] = new
            total[h] = fade * total[h] + jnp.sum(parts[0] + parts[1], axis=1, keepdims=True)
            summed[h] = (
                fade * summed[h]
                + jnp.dot(parts[0].astype(jnp.bfloat16), kv[a, 1], preferred_element_type=jnp.float32)
                + jnp.dot(parts[1].astype(jnp.bfloat16), kv[b, 1], preferred_element_type=jnp.float32)
            )

    @pl.when(core == 1)
    def _():
        for k in range(1, hops // FAR + 1):
            for way in (0, 1):
                if FAR * k <= reach[way]:
                    wkv_arrival(way, FAR * k).wait_recv()
                    wkv_send(way, FAR * k)
                    wkv_twin(way, FAR * k).start()
            for d in range(FAR * (k - 1) + 1, FAR * k):
                for way in (0, 1):
                    wkv_arrival(way, d).wait_recv()
                    wkv_twin(way, d).start()
        w_own_sends(1)
        for d in range(1, chips):
            normed_from(d).wait_recv()
        for d in range(chips):
            normed_from_mate(d).wait_recv()
        incoming = wkv.at[pl.ds(0, n - 1), pl.ds(0, wkv_half), :]
        remote(incoming, incoming, twin_ss.at[2], twin_rs.at[2], mate).wait_recv()
        projected = jnp.dot(
            normed[...].reshape(rows, width),
            wkv[...].reshape(width, 2 * HEAD),
            preferred_element_type=jnp.float32,
        )
        kv[z, 0] = turned(projected[:, :HEAD], kg[...]).astype(jnp.bfloat16)
        kv[z, 1] = projected[:, HEAD:].astype(jnp.bfloat16)
        for c in range(CHUNKS):
            kv_ring(0, z, 0, c).start()
            kv_ring(1, z, 0, c).start()
        for c in range(CHUNKS):
            kv_mate(0, z, 0, c).start()
        for d in range(1, chips):
            normed_mate(d).start()

        def kv_step(s):
            for c in range(CHUNKS):
                kv_ring(0, back(s), s - 1, c).wait_recv()
                kv_ring(0, back(s), s, c).start()
                kv_mate(0, back(s), s, c).start()
                kv_ring(1, ahead(s), s - 1, c).wait_recv()

                @pl.when(s < hops - 1)
                def _():
                    kv_ring(1, ahead(s), s, c).start()

                kv_mate(1, ahead(s), s, c).start()

        def early(s, carry):
            kv_step(s)
            return carry

        lax.fori_loop(1, LEAD + 1, early, 0)
        for h in range(heads):
            kv_step(LEAD + 1 + h)
            if h == 0:
                incoming = several(0, n - 1, 0)
                remote(incoming, incoming, md_ss.at[0], md_rs.at[0], mate).wait_recv()
                query_weights_here()
            make_queries(h, 1)
        lead = LEAD + heads
        pace = -(-(hops - 1) // (hops - 1 - lead))

        def pair(i, carry):
            attend(back(i), ahead(i))
            return carry

        def late(s, carry):
            kv_step(s)
            first = jnp.minimum(pace * (s - 1 - lead), s - 1) + 1
            lax.fori_loop(first, jnp.minimum(pace * (s - lead), s) + 1, pair, 0)
            return carry

        lax.fori_loop(lead + 1, hops, late, 0)
        for c in range(CHUNKS):
            kv_ring(0, back(hops), hops - 1, c).wait_recv()
            kv_mate(0, back(hops), hops, c).start()
        attend(z, back(hops))
        incoming = several(1, n - 1, 0)
        remote(incoming, incoming, md_ss.at[1], md_rs.at[1], mate).wait_recv()

    @pl.when(core == 0)
    def _():
        def w_step(f, k):
            w_arrival(f, 0, k - 1, MID).wait_recv()
            w_ring(f, 0, k, MID).start()
            w_ring(f, 0, k, 1).start()
            w_share(f, 0, MID * k)
            w_arrival(f, 1, k - 1, MID).wait_recv()

            @pl.when(MID * (k + 1) < hops)
            def _():
                w_ring(f, 1, k, MID).start()

            w_ring(f, 1, k, 1).start()
            w_share(f, 1, MID * k)
            for way in (0, 1):
                w_arrival(f, way, k - 1, 1).wait_recv()
                w_share(f, way, MID * k - 1)

        def w_end(f):
            k = hops // MID
            w_arrival(f, 0, k - 1, MID).wait_recv()
            w_share(f, 0, MID * k)
            for way in (0, 1):
                w_arrival(f, way, k - 1, 1).wait_recv()
                w_share(f, way, MID * k - 1)

        def query_step(k, carry):
            w_step(0, k)
            return carry

        def both_step(k, carry):
            w_step(0, k)
            w_step(1, k - middle + 1)
            return carry

        last = hops // MID
        middle = last // 2
        lax.fori_loop(1, middle - 1, query_step, 0)
        for d in range(1, chips):
            normed_from(d).wait_recv()
            normed_mate(d).start()
        w_step(0, middle - 1)
        w_own_sends(1)
        lax.fori_loop(middle, last, both_step, 0)
        w_end(0)
        for d in range(chips):
            normed_from_mate(d).wait_recv()
        query_weights_here()
        make_queries(0, heads)

        def pair(s, carry):
            kv_from_mate(0, back(s), s).wait_recv()
            kv_from_mate(1, ahead(s), s).wait_recv()
            attend(back(s), ahead(s))
            return carry

        def out_step(k, carry):
            w_step(1, k)
            return lax.fori_loop(2 * (k - done) - 1, 2 * (k - done) + 1, pair, carry)

        done = last - middle
        lax.fori_loop(done + 1, last, out_step, 0)
        w_end(1)
        lax.fori_loop(2 * (last - 1 - done) + 1, hops, pair, 0)
        kv_from_mate(0, z, 0).wait_recv()
        kv_from_mate(0, back(hops), hops).wait_recv()
        attend(z, back(hops))

    attended = jnp.concatenate([(summed[h] / total[h]).astype(jnp.bfloat16) for h in range(heads)], axis=1)
    incoming = several(1, n - 1, 0)
    remote(incoming, incoming, twin_ss.at[1], twin_rs.at[1], mate).wait_recv()

    per_piece = n // QUARTERS

    def term_mate(p):
        return remote(terms.at[p, 1 - core], partner_terms.at[p], td_ss.at[p], td_rs.at[p], mate)

    def project(p, carry):
        for j in range(per_piece // 2):
            first = p * per_piece + 2 * j
            both = jnp.concatenate([wo[first, core], wo[first + 1, core]], axis=1)
            term = jnp.dot(attended, both, preferred_element_type=jnp.float32).astype(jnp.bfloat16)
            for owner in range(n_tp):
                terms[p, owner % 2, owner // 2, :, 2 * j * cols : (2 * j + 2) * cols] = term[
                    owner * own_rows : (owner + 1) * own_rows
                ]
        term_mate(p).start()
        return carry

    lax.fori_loop(0, QUARTERS, project, 0)

    near = own_rows // 2
    upper, lower = pl.ds(0, near), pl.ds(near, near)
    ways = ((1, upper, lower), (chips - 1, lower, upper))

    def pair_sum(p, there, part):
        return terms[p, core, there, part].astype(jnp.float32) + partner_terms[p, there, part].astype(jnp.float32)

    def x_send(src, dst, p, way, i):
        return remote(src, dst, x_ss.at[p, way, i], x_rs.at[p, way, i], across[ways[way][0] - 1])

    def far_part(p, way):
        return x_send(pair_sums.at[p, way, 0], relayed.at[p, way], p, way, 0)

    def near_part(p, way):
        return x_send(pair_sums.at[p, way, 1], arrived.at[p, way, ways[way][2]], p, way, 1)

    def passed_part(p, way):
        return x_send(pair_sums.at[p, way, 2], arrived.at[p, way, ways[way][1]], p, way, 2)

    def send_sums(p):
        term_mate(p).wait_recv()
        for way, (on, passed, kept) in enumerate(ways):
            pair_sums[p, way, 0] = pair_sum(p, lax.rem(x + 2, chips), passed).astype(jnp.bfloat16)
            far_part(p, way).start()
        for way, (on, passed, kept) in enumerate(ways):
            pair_sums[p, way, 1] = pair_sum(p, lax.rem(x + on, chips), kept).astype(jnp.bfloat16)
            near_part(p, way).start()

    def pass_on(p):
        for way, (on, passed, kept) in enumerate(ways):
            far_part(p, way).wait_recv()
            both = pair_sum(p, lax.rem(x + on, chips), passed) + relayed[p, way].astype(jnp.float32)
            pair_sums[p, way, 2] = both.astype(jnp.bfloat16)
            passed_part(p, way).start()

    send_sums(0)
    for p in range(1, QUARTERS):
        send_sums(p)
        pass_on(p - 1)
    pass_on(QUARTERS - 1)
    piece_cols = per_piece * cols

    def out_copy(p):
        part = pl.ds(p * piece_cols, piece_cols)
        return pltpu.make_async_copy(mixed.at[:, part], out_hbm.at[:, part], out_sems.at[p])

    for p in range(QUARTERS):
        for way in (0, 1):
            near_part(p, way).wait_recv()
            passed_part(p, way).wait_recv()
        rows_sum = pair_sum(p, x, pl.ds(0, own_rows))
        for way in (0, 1):
            rows_sum = rows_sum + arrived[p, way].astype(jnp.float32)
        mixed[:, p * piece_cols : (p + 1) * piece_cols] = rows_sum.astype(mixed.dtype)
        out_copy(p).start()

    for p in range(QUARTERS):
        out_copy(p).wait()
    for d in range(1, chips):
        normed_to(d).wait_send()
    for d in range(chips):
        normed_mate(d).wait_send()

    @pl.when(core == 1)
    def _():
        for way in (0, 1):
            sends = sum(1 for d in range(0, reach[way], FAR) for j in range(1, FAR + 1) if d + j <= reach[way])
            sent = wkv.at[pl.ds(0, sends), pl.ds(0, wkv_half), :]
            remote(sent, sent, wkv_ss.at[way], wkv_rs.at[way, 0, 0], mate).wait_send()
            sent = kv.at[pl.ds(0, reach[way])]
            remote(sent, sent, kv_ss.at[way], kv_rs.at[way, 0, 0], mate).wait_send()
        sent = wkv.at[pl.ds(0, n - 1), pl.ds(0, wkv_half), :]
        remote(sent, sent, twin_ss.at[2], twin_rs.at[2], mate).wait_send()
        remote(kv, kv, kd_ss.at[0], kd_rs.at[0, 0], mate).wait_send()
        for f in (0, 1):
            sent = several(f, 2 * MID, 0)
            remote(sent, sent, w_ss.at[f], w_rs.at[f, 0, 0, 0], mate).wait_send()

    @pl.when(core == 0)
    def _():
        for f in (0, 1):
            sent = several(f, n - 1 - 2 * MID + MID)
            remote(sent, sent, w_ss.at[f], w_rs.at[f, 0, 0, 0], mate).wait_send()
            sent = several(f, n - 1)
            remote(sent, sent, twin_ss.at[f], twin_rs.at[f], mate).wait_send()
            sent = several(f, n - 1, 0)
            remote(sent, sent, md_ss.at[f], md_rs.at[f], mate).wait_send()

    for p in range(QUARTERS):
        term_mate(p).wait_send()
        for way in (0, 1):
            far_part(p, way).wait_send()
            near_part(p, way).wait_send()
            passed_part(p, way).wait_send()


def solution(mesh):
    n, n_tp = mesh.shape["sp"], mesh.shape["tp"]

    def local(tokens, input_gain, w_query, w_key, w_value, query_gain, key_gain, w_out):
        own_rows, width = tokens.shape
        rows = own_rows * n_tp
        depth, q_cols = w_query.shape
        heads = q_cols // HEAD
        out_rows, cols = w_out.shape
        chips = n_tp // 2
        hops = n // 2
        piece_cols = width // QUARTERS
        quarter = HEAD // 4
        inverse = 10000.0 ** (-np.arange(quarter) * 2.0 / (2 * quarter))
        inverse = jnp.asarray(np.tile(inverse, 4)[None, :].astype(np.float32))
        bf16, f32 = jnp.bfloat16, jnp.float32
        dma = pltpu.SemaphoreType.DMA
        return pl.pallas_call(
            functools.partial(fused, (n, n_tp)),
            out_shape=jax.ShapeDtypeStruct((own_rows, width), bf16),
            in_specs=[pl.BlockSpec(memory_space=pltpu.HBM)] * 9,
            out_specs=pl.BlockSpec(memory_space=pltpu.HBM),
            scratch_shapes=[
                pltpu.VMEM((own_rows, width), bf16),
                pltpu.VMEM((own_rows, width), bf16),
                pltpu.VMEM((1, width), f32),
                pltpu.VMEM((1, HEAD), f32),
                pltpu.VMEM((1, HEAD), f32),
                pltpu.VMEM((1, HEAD), f32),
                pltpu.VMEM((n_tp, own_rows, width), bf16),
                pltpu.VMEM((n, depth, 2 * HEAD), bf16),
                pltpu.VMEM((n, 2, depth, q_cols), bf16),
                pltpu.VMEM((n, 2, out_rows, cols), bf16),
                pltpu.VMEM((n, 2, rows, HEAD), bf16),
                pltpu.VMEM((rows, HEAD), f32),
                pltpu.VMEM((rows, HEAD), f32),
                pltpu.VMEM((heads, rows, HEAD), bf16),
                pltpu.VMEM((heads, rows, HEAD), f32),
                pltpu.VMEM((heads, rows, HEAD), f32),
                pltpu.VMEM((heads, rows, HEAD), f32),
                pltpu.VMEM((QUARTERS, 2, chips, own_rows, piece_cols), bf16),
                pltpu.VMEM((QUARTERS, chips, own_rows, piece_cols), bf16),
                pltpu.VMEM((QUARTERS, 2, 3, own_rows // 2, piece_cols), bf16),
                pltpu.VMEM((QUARTERS, 2, own_rows // 2, piece_cols), bf16),
                pltpu.VMEM((QUARTERS, 2, own_rows, piece_cols), bf16),
                dma((9,)),
                dma((QUARTERS,)),
                dma((chips - 1,)),
                dma((chips - 1,)),
                dma((chips,)),
                dma((chips,)),
                dma((2,)),
                dma((2, hops // FAR, FAR)),
                dma((2,)),
                dma((2, 2, hops // MID, MID)),
                dma((3,)),
                dma((3,)),
                dma((2,)),
                dma((2,)),
                dma((2,)),
                dma((2, hops, CHUNKS)),
                dma((1,)),
                dma((2, hops + 1)),
                dma((QUARTERS,)),
                dma((QUARTERS,)),
                dma((QUARTERS, 2, 3)),
                dma((QUARTERS, 2, 3)),
            ],
            compiler_params=pltpu.CompilerParams(
                collective_id=0, has_side_effects=True, vmem_limit_bytes=56 * 1024 * 1024
            ),
        )(
            tokens,
            input_gain[None, :],
            w_query,
            w_key,
            w_value,
            query_gain[None, :],
            key_gain[None, :],
            w_out,
            inverse,
        )

    in_specs = (
        P(("grp", "sp", "tp"), None),
        P(),
        P("sp", "tp"),
        P("sp", None),
        P("sp", None),
        P(),
        P(),
        P("tp", "sp"),
    )
    out_specs = P(("grp", "sp", "tp"), None)
    return jax.shard_map(local, mesh=mesh, in_specs=in_specs, out_specs=out_specs, check_vma=False)
```

```python
import functools

import jax
import jax.numpy as jnp
import numpy as np
from jax import lax
from jax.experimental import pallas as pl
from jax.experimental.pallas import tpu as pltpu
from jax.sharding import PartitionSpec as P

HEAD = 128
GRID_W = 64
EPS = 1e-06
CHUNKS = 4
FAR = 4
MID = 2
LEAD = 6
QUARTERS = 4
MESH = pl.DeviceIdType.MESH


def remote(src, dst, send_sem, recv_sem, device):
    return pltpu.make_async_remote_copy(
        src_ref=src, dst_ref=dst, send_sem=send_sem, recv_sem=recv_sem, device_id=device, device_id_type=MESH
    )


def fused(
    sizes,
    tok_hbm,
    gain_hbm,
    wq_hbm,
    wk_hbm,
    wv_hbm,
    qg_hbm,
    kg_hbm,
    wo_hbm,
    inv_hbm,
    out_hbm,
    mixed,
    tok,
    gain,
    qg,
    kg,
    inv,
    normed,
    wkv,
    wq,
    wo,
    kv,
    cosine,
    sine,
    queries,
    peak,
    total,
    summed,
    terms,
    partner_terms,
    pair_sums,
    relayed,
    arrived,
    in_sems,
    out_sems,
    left_sem,
    nx_ss,
    nx_rs,
    nd_ss,
    nd_rs,
    wkv_ss,
    wkv_rs,
    w_ss,
    w_rs,
    twin_ss,
    twin_rs,
    md_ss,
    md_rs,
    kv_ss,
    kv_rs,
    kd_ss,
    kd_rs,
    td_ss,
    td_rs,
    x_ss,
    x_rs,
):
    n, n_tp = sizes
    chips = n_tp // 2
    hops = n // 2
    grp, z, t = lax.axis_index("grp"), lax.axis_index("sp"), lax.axis_index("tp")
    x, core = t // 2, t % 2
    half = grp % 2
    other_t = t + 1 - 2 * core
    low_t = t - core
    mate = {"tp": other_t}
    other_grp = grp + 1 - 2 * half
    across = [{"tp": lax.rem(t + 2 * d, n_tp)} for d in range(1, chips)]

    own_rows, width = tok.shape
    rows = own_rows * n_tp
    q_cols = wq.shape[3]
    heads = q_cols // HEAD
    cols = wo.shape[3]

    def back(s):
        return lax.rem(z - s + n, n)

    def ahead(s):
        return lax.rem(z + s, n)

    def toward(way, j):
        return ahead(j) if way == 0 else back(j)

    def source(way, d):
        return back(d) if way == 0 else ahead(d)

    columns = pl.ds(pl.multiple_of(x * HEAD, HEAD), HEAD)
    loads = [
        pltpu.make_async_copy(source_ref, target, in_sems.at[i])
        for i, (source_ref, target) in enumerate(
            (
                (wk_hbm.at[:, columns], wkv.at[z, :, pl.ds(0, HEAD)]),
                (wv_hbm.at[:, columns], wkv.at[z, :, pl.ds(HEAD, HEAD)]),
                (tok_hbm, tok),
                (gain_hbm, gain),
                (wq_hbm, wq.at[z, core]),
                (wo_hbm, wo.at[z, core]),
                (qg_hbm, qg),
                (kg_hbm, kg),
                (inv_hbm, inv),
            )
        )
    ]
    for load in loads:
        load.start()

    barrier = pltpu.get_barrier_semaphore()

    def say(semaphore, peers):
        for peer in peers:
            pl.semaphore_signal(semaphore, inc=1, device_id=peer, device_id_type=MESH)

    level = [mate, {"grp": other_grp}, {"grp": other_grp, "tp": other_t}] + across
    say(barrier, level)

    def neighbours(way):
        same = [{"sp": toward(way, j)} for j in range(1, FAR + 1)]
        other = [{"sp": toward(way, j), "tp": other_t} for j in range(1, MID + 1)]
        return same, other

    def greet(way, semaphore, also):
        same, other = neighbours(way)

        @pl.when(core == 1)
        def _():
            say(semaphore, same + other[:also])

        @pl.when(core == 0)
        def _():
            say(semaphore, same[:MID] + other)

    greet(1, barrier, MID)
    pl.semaphore_wait(barrier, len(level) + 2 * MID + core * (FAR - MID))
    greet(0, left_sem, 0)

    def left_is_in():
        pl.semaphore_wait(left_sem, MID + core * FAR)

    wkv_half = wkv.shape[1] // 2

    def wkv_piece(slot):
        return wkv.at[slot, pl.ds(pl.multiple_of(half * wkv_half, wkv_half), wkv_half), :]

    def wkv_ring(way, d, j):
        piece = wkv_piece(source(way, d))
        return remote(piece, piece, wkv_ss.at[way], wkv_rs.at[way, d // FAR, j - 1], {"sp": toward(way, j)})

    def wkv_arrival(way, d):
        piece = wkv_piece(source(way, d))
        return remote(
            piece, piece, wkv_ss.at[way], wkv_rs.at[way, (d - 1) // FAR, (d - 1) % FAR], {"sp": toward(way, 1)}
        )

    def wkv_twin(way, d):
        piece = wkv_piece(source(way, d))
        return remote(piece, piece, twin_ss.at[2], twin_rs.at[2], {"grp": other_grp})

    reach = (hops, hops - 1)

    def wkv_send(way, d):
        for j in [FAR] + list(range(1, FAR)):
            if d + j <= reach[way]:
                wkv_ring(way, d, j).start()

    weights = (wq, wo)

    def half_rows(f):
        size = weights[f].shape[2] // 2
        return pl.ds(pl.multiple_of(half * size, size), size)

    def w_piece(f, slot):
        return weights[f].at[slot, :, half_rows(f), :]

    def w_own(f, way, j):
        piece = weights[f].at[z, core, half_rows(f), :]
        return remote(piece, piece, w_ss.at[f], w_rs.at[f, way, 0, j - 1], {"sp": toward(way, j), "tp": low_t})

    def w_ring(f, way, k, j):
        piece = w_piece(f, source(way, MID * k))
        return remote(piece, piece, w_ss.at[f], w_rs.at[f, way, k, j - 1], {"sp": toward(way, j)})

    def w_arrival(f, way, k, j):
        piece = w_piece(f, source(way, MID * k + j))
        return remote(piece, piece, w_ss.at[f], w_rs.at[f, way, k, j - 1], {"sp": toward(way, 1)})

    def w_share(f, way, d):
        slot = source(way, d)
        for c in (0, 1):
            piece = weights[f].at[slot, c, half_rows(f), :]
            remote(piece, piece, twin_ss.at[f], twin_rs.at[f], {"grp": other_grp, "tp": low_t + c}).start()
        piece = weights[f].at[slot, 1, half_rows(f), :]
        remote(piece, piece, md_ss.at[f], md_rs.at[f], mate).start()

    def several(f, count, c=None):
        size = weights[f].shape[2] // 2
        if c is None:
            return weights[f].at[pl.ds(0, count), :, pl.ds(0, size), :]
        return weights[f].at[pl.ds(0, count), c, pl.ds(0, size), :]

    chunk = 2 * rows // CHUNKS

    def kv_piece(slot, c):
        return kv.at[slot, c * chunk // rows, pl.ds(c * chunk % rows, chunk), :]

    def kv_ring(way, slot, s, c):
        piece = kv_piece(slot, c)
        return remote(piece, piece, kv_ss.at[way], kv_rs.at[way, s, c], {"sp": toward(way, 1)})

    def kv_mate(way, slot, s, c):
        piece = kv_piece(slot, c)
        return remote(piece, piece, kd_ss.at[0], kd_rs.at[way, s], mate)

    def kv_from_mate(way, slot, s):
        return remote(kv.at[slot], kv.at[slot], kd_ss.at[0], kd_rs.at[way, s], mate)

    def normed_to(d):
        return remote(normed.at[t], normed.at[t], nx_ss.at[d - 1], nx_rs.at[d - 1], across[d - 1])

    def normed_slot(d, of):
        return normed.at[lax.rem(of + n_tp - 2 * d, n_tp)]

    def normed_mate(d):
        return remote(normed_slot(d, t), normed_slot(d, t), nd_ss.at[d], nd_rs.at[d], mate)

    def normed_from(d):
        return remote(normed_slot(d, t), normed_slot(d, t), nx_ss.at[d - 1], nx_rs.at[d - 1], across[d - 1])

    def normed_from_mate(d):
        return remote(normed_slot(d, other_t), normed_slot(d, other_t), nd_ss.at[d], nd_rs.at[d], mate)

    loads[0].wait()
    loads[1].wait()

    @pl.when(core == 1)
    def _():
        wkv_send(0, 0)

    loads[2].wait()
    loads[3].wait()
    floats = tok[...].astype(jnp.float32)
    scale = lax.rsqrt(jnp.mean(floats * floats, axis=-1, keepdims=True) + EPS)
    normed[t] = (floats * scale * gain[...]).astype(jnp.bfloat16)
    for d in range(1, chips):
        normed_to(d).start()
    normed_mate(0).start()

    def w_own_sends(f, way):
        for j in range(MID, 0, -1):
            w_own(f, way, j).start()

    loads[4].wait()
    w_own_sends(0, 0)
    left_is_in()

    @pl.when(core == 1)
    def _():
        wkv_send(1, 0)

    w_own_sends(0, 1)
    for load in loads[5:]:
        load.wait()

    lane = lax.broadcasted_iota(jnp.int32, (rows, HEAD), 1)
    place = lax.broadcasted_iota(jnp.int32, (rows, HEAD), 0) + z * rows
    spot = jnp.where(lane < HEAD // 2, place // GRID_W, place % GRID_W).astype(jnp.float32)
    angles = spot * inv[...]
    first_half = lane % (HEAD // 2) < HEAD // 4
    cosine[...] = jnp.cos(angles)
    sine[...] = jnp.where(first_half, -jnp.sin(angles), jnp.sin(angles))
    peak[...] = jnp.full_like(peak, -1e30)
    total[...] = jnp.zeros_like(total)
    summed[...] = jnp.zeros_like(summed)

    def turned(raw, head_gain):
        heads_in = raw.astype(jnp.bfloat16).astype(jnp.float32)
        scale = lax.rsqrt(jnp.mean(heads_in * heads_in, axis=-1, keepdims=True) + EPS)
        scaled = heads_in * scale * head_gain
        lanes = lax.broadcasted_iota(jnp.int32, scaled.shape, 1)
        other = jnp.where(
            lanes % (HEAD // 2) < HEAD // 4,
            pltpu.roll(scaled, HEAD - HEAD // 4, 1),
            pltpu.roll(scaled, HEAD // 4, 1),
        )
        return scaled * cosine[...] + other * sine[...]

    def query_weights_here():
        incoming = several(0, n - 1, 0)
        remote(incoming, incoming, twin_ss.at[0], twin_rs.at[0], mate).wait_recv()

    def make_queries(first, count):
        raw = jnp.dot(
            normed[...].reshape(rows, width),
            wq[:, core, :, first * HEAD : (first + count) * HEAD].reshape(width, count * HEAD),
            preferred_element_type=jnp.float32,
        )
        for h in range(count):
            queries[first + h] = (turned(raw[:, h * HEAD : (h + 1) * HEAD], qg[...]) * HEAD ** (-0.5)).astype(
                jnp.bfloat16
            )

    def attend(a, b):
        pieces = [(h, pl.ds(r, HEAD)) for h in range(heads) for r in range(0, rows, HEAD)]
        scores = [
            [
                lax.dot_general(
                    queries[h, part], kv[i, 0], (((1,), (1,)), ((), ())), preferred_element_type=jnp.float32
                )
                for i in (a, b)
            ]
            for h, part in pieces
        ]
        peaks = []
        for (h, part), pair in zip(pieces, scores):
            highest = jnp.maximum(*pair)
            highest = functools.reduce(
                jnp.maximum, [highest[:, i : i + HEAD] for i in range(0, rows, HEAD)]
            )
            peaks.append(jnp.maximum(peak[h, part], jnp.max(highest, axis=1, keepdims=True)))
        for (h, part), pair, new in zip(pieces, scores, peaks):
            fade = jnp.exp(peak[h, part] - new)
            wide = jnp.concatenate([new] * (rows // HEAD), axis=1)
            parts = [jnp.exp(score - wide) for score in pair]
            peak[h, part] = new
            added = parts[0] + parts[1]
            total[h, part] = fade * total[h, part] + sum(added[:, i : i + HEAD] for i in range(0, rows, HEAD))
            summed[h, part] = (
                fade * summed[h, part]
                + jnp.dot(parts[0].astype(jnp.bfloat16), kv[a, 1], preferred_element_type=jnp.float32)
                + jnp.dot(parts[1].astype(jnp.bfloat16), kv[b, 1], preferred_element_type=jnp.float32)
            )

    @pl.when(core == 1)
    def _():
        for k in range(1, hops // FAR + 1):
            for way in (0, 1):
                if FAR * k <= reach[way]:
                    wkv_arrival(way, FAR * k).wait_recv()
                    wkv_send(way, FAR * k)
                    wkv_twin(way, FAR * k).start()
            for d in range(FAR * (k - 1) + 1, FAR * k):
                for way in (0, 1):
                    wkv_arrival(way, d).wait_recv()
                    wkv_twin(way, d).start()
        w_own_sends(1, 0)
        w_own_sends(1, 1)
        for d in range(1, chips):
            normed_from(d).wait_recv()
        for d in range(chips):
            normed_from_mate(d).wait_recv()
        incoming = wkv.at[pl.ds(0, n - 1), pl.ds(0, wkv_half), :]
        remote(incoming, incoming, twin_ss.at[2], twin_rs.at[2], mate).wait_recv()
        projected = jnp.dot(
            normed[...].reshape(rows, width),
            wkv[...].reshape(width, 2 * HEAD),
            preferred_element_type=jnp.float32,
        )
        kv[z, 0] = turned(projected[:, :HEAD], kg[...]).astype(jnp.bfloat16)
        kv[z, 1] = projected[:, HEAD:].astype(jnp.bfloat16)
        for c in range(CHUNKS):
            kv_ring(0, z, 0, c).start()
            kv_ring(1, z, 0, c).start()
        for c in range(CHUNKS):
            kv_mate(0, z, 0, c).start()
        for d in range(1, chips):
            normed_mate(d).start()

        def kv_step(s):
            for c in range(CHUNKS):
                kv_ring(0, back(s), s - 1, c).wait_recv()
                kv_ring(0, back(s), s, c).start()
                kv_mate(0, back(s), s, c).start()
                kv_ring(1, ahead(s), s - 1, c).wait_recv()

                @pl.when(s < hops - 1)
                def _():
                    kv_ring(1, ahead(s), s, c).start()

                kv_mate(1, ahead(s), s, c).start()

        def early(s, carry):
            kv_step(s)
            return carry

        lax.fori_loop(1, LEAD + 1, early, 0)
        for h in range(heads):
            kv_step(LEAD + 1 + h)
            if h == 0:
                incoming = several(0, n - 1, 0)
                remote(incoming, incoming, md_ss.at[0], md_rs.at[0], mate).wait_recv()
                query_weights_here()
            make_queries(h, 1)
        lead = LEAD + heads
        pace = -(-(hops - 1) // (hops - 1 - lead))

        def pair(i, carry):
            attend(back(i), ahead(i))
            return carry

        def late(s, carry):
            kv_step(s)
            first = jnp.minimum(pace * (s - 1 - lead), s - 1) + 1
            lax.fori_loop(first, jnp.minimum(pace * (s - lead), s) + 1, pair, 0)
            return carry

        lax.fori_loop(lead + 1, hops, late, 0)
        for c in range(CHUNKS):
            kv_ring(0, back(hops), hops - 1, c).wait_recv()
            kv_mate(0, back(hops), hops, c).start()
        attend(z, back(hops))
        incoming = several(1, n - 1, 0)
        remote(incoming, incoming, md_ss.at[1], md_rs.at[1], mate).wait_recv()

    @pl.when(core == 0)
    def _():
        def w_step(f, k, share=w_share):
            w_arrival(f, 0, k - 1, MID).wait_recv()
            w_ring(f, 0, k, MID).start()
            w_ring(f, 0, k, 1).start()
            share(f, 0, MID * k)
            w_arrival(f, 1, k - 1, MID).wait_recv()

            @pl.when(MID * (k + 1) < hops)
            def _():
                w_ring(f, 1, k, MID).start()

            w_ring(f, 1, k, 1).start()
            share(f, 1, MID * k)
            for way in (0, 1):
                w_arrival(f, way, k - 1, 1).wait_recv()
                share(f, way, MID * k - 1)

        def w_end(f):
            k = hops // MID
            w_arrival(f, 0, k - 1, MID).wait_recv()
            w_share(f, 0, MID * k)
            for way in (0, 1):
                w_arrival(f, way, k - 1, 1).wait_recv()
                w_share(f, way, MID * k - 1)

        def query_step(k, carry):
            w_step(0, k, lambda f, way, d: None)
            return carry

        def both_step(k, carry):
            w_step(0, k)
            w_step(1, k - middle + 1)
            return carry

        last = hops // MID
        middle = last // 2
        lax.fori_loop(1, middle - 1, query_step, 0)
        for d in range(1, chips):
            normed_from(d).wait_recv()
            normed_mate(d).start()
        query_step(middle - 1, 0)
        w_own_sends(1, 0)
        w_own_sends(1, 1)
        for d in range(1, MID * middle - MID + 1):
            for way in (0, 1):
                w_share(0, way, d)
        lax.fori_loop(middle, last, both_step, 0)
        w_end(0)
        for d in range(chips):
            normed_from_mate(d).wait_recv()
        query_weights_here()
        make_queries(0, heads)

        def pair(s, carry):
            kv_from_mate(0, back(s), s).wait_recv()
            kv_from_mate(1, ahead(s), s).wait_recv()
            attend(back(s), ahead(s))
            return carry

        def out_step(k, carry):
            w_step(1, k)
            return lax.fori_loop(2 * (k - done) - 1, 2 * (k - done) + 1, pair, carry)

        done = last - middle
        lax.fori_loop(done + 1, last, out_step, 0)
        w_end(1)
        lax.fori_loop(2 * (last - 1 - done) + 1, hops, pair, 0)
        kv_from_mate(0, z, 0).wait_recv()
        kv_from_mate(0, back(hops), hops).wait_recv()
        attend(z, back(hops))

    attended = jnp.concatenate(
        [
            (summed[h] / jnp.sum(total[h], axis=1, keepdims=True)).astype(jnp.bfloat16)
            for h in range(heads)
        ],
        axis=1,
    )
    incoming = several(1, n - 1, 0)
    remote(incoming, incoming, twin_ss.at[1], twin_rs.at[1], mate).wait_recv()

    per_piece = n // QUARTERS

    def term_mate(p):
        return remote(terms.at[p, 1 - core], partner_terms.at[p], td_ss.at[p], td_rs.at[p], mate)

    def project(p, carry):
        for j in range(per_piece // 2):
            first = p * per_piece + 2 * j
            both = jnp.concatenate([wo[first, core], wo[first + 1, core]], axis=1)
            term = jnp.dot(attended, both, preferred_element_type=jnp.float32).astype(jnp.bfloat16)
            for owner in range(n_tp):
                terms[p, owner % 2, owner // 2, :, 2 * j * cols : (2 * j + 2) * cols] = term[
                    owner * own_rows : (owner + 1) * own_rows
                ]
        term_mate(p).start()
        return carry

    lax.fori_loop(0, QUARTERS, project, 0)

    near = own_rows // 2
    upper, lower = pl.ds(0, near), pl.ds(near, near)
    ways = ((1, upper, lower), (chips - 1, lower, upper))

    def pair_sum(p, there, part):
        return terms[p, core, there, part].astype(jnp.float32) + partner_terms[p, there, part].astype(jnp.float32)

    def x_send(src, dst, p, way, i):
        return remote(src, dst, x_ss.at[p, way, i], x_rs.at[p, way, i], across[ways[way][0] - 1])

    def far_part(p, way):
        return x_send(pair_sums.at[p, way, 0], relayed.at[p, way], p, way, 0)

    def near_part(p, way):
        return x_send(pair_sums.at[p, way, 1], arrived.at[p, way, ways[way][2]], p, way, 1)

    def passed_part(p, way):
        return x_send(pair_sums.at[p, way, 2], arrived.at[p, way, ways[way][1]], p, way, 2)

    def send_sums(p):
        term_mate(p).wait_recv()
        for way, (on, passed, kept) in enumerate(ways):
            pair_sums[p, way, 0] = pair_sum(p, lax.rem(x + 2, chips), passed).astype(jnp.bfloat16)
            far_part(p, way).start()
        for way, (on, passed, kept) in enumerate(ways):
            pair_sums[p, way, 1] = pair_sum(p, lax.rem(x + on, chips), kept).astype(jnp.bfloat16)
            near_part(p, way).start()

    def pass_on(p):
        for way, (on, passed, kept) in enumerate(ways):
            far_part(p, way).wait_recv()
            both = pair_sum(p, lax.rem(x + on, chips), passed) + relayed[p, way].astype(jnp.float32)
            pair_sums[p, way, 2] = both.astype(jnp.bfloat16)
            passed_part(p, way).start()

    send_sums(0)
    for p in range(1, QUARTERS):
        send_sums(p)
        pass_on(p - 1)
    pass_on(QUARTERS - 1)
    piece_cols = per_piece * cols

    def out_copy(p):
        part = pl.ds(p * piece_cols, piece_cols)
        return pltpu.make_async_copy(mixed.at[:, part], out_hbm.at[:, part], out_sems.at[p])

    for p in range(QUARTERS):
        for way in (0, 1):
            near_part(p, way).wait_recv()
            passed_part(p, way).wait_recv()
        rows_sum = pair_sum(p, x, pl.ds(0, own_rows))
        for way in (0, 1):
            rows_sum = rows_sum + arrived[p, way].astype(jnp.float32)
        mixed[:, p * piece_cols : (p + 1) * piece_cols] = rows_sum.astype(mixed.dtype)
        out_copy(p).start()

    for p in range(QUARTERS):
        out_copy(p).wait()
    for d in range(1, chips):
        normed_to(d).wait_send()
    for d in range(chips):
        normed_mate(d).wait_send()

    @pl.when(core == 1)
    def _():
        for way in (0, 1):
            sends = sum(1 for d in range(0, reach[way], FAR) for j in range(1, FAR + 1) if d + j <= reach[way])
            sent = wkv.at[pl.ds(0, sends), pl.ds(0, wkv_half), :]
            remote(sent, sent, wkv_ss.at[way], wkv_rs.at[way, 0, 0], mate).wait_send()
            sent = kv.at[pl.ds(0, reach[way])]
            remote(sent, sent, kv_ss.at[way], kv_rs.at[way, 0, 0], mate).wait_send()
        sent = wkv.at[pl.ds(0, n - 1), pl.ds(0, wkv_half), :]
        remote(sent, sent, twin_ss.at[2], twin_rs.at[2], mate).wait_send()
        remote(kv, kv, kd_ss.at[0], kd_rs.at[0, 0], mate).wait_send()
        for f in (0, 1):
            sent = several(f, 2 * MID, 0)
            remote(sent, sent, w_ss.at[f], w_rs.at[f, 0, 0, 0], mate).wait_send()

    @pl.when(core == 0)
    def _():
        for f in (0, 1):
            sent = several(f, n - 1 - 2 * MID + MID)
            remote(sent, sent, w_ss.at[f], w_rs.at[f, 0, 0, 0], mate).wait_send()
            sent = several(f, n - 1)
            remote(sent, sent, twin_ss.at[f], twin_rs.at[f], mate).wait_send()
            sent = several(f, n - 1, 0)
            remote(sent, sent, md_ss.at[f], md_rs.at[f], mate).wait_send()

    for p in range(QUARTERS):
        term_mate(p).wait_send()
        for way in (0, 1):
            far_part(p, way).wait_send()
            near_part(p, way).wait_send()
            passed_part(p, way).wait_send()


def solution(mesh):
    n, n_tp = mesh.shape["sp"], mesh.shape["tp"]

    def local(tokens, input_gain, w_query, w_key, w_value, query_gain, key_gain, w_out):
        own_rows, width = tokens.shape
        rows = own_rows * n_tp
        depth, q_cols = w_query.shape
        heads = q_cols // HEAD
        out_rows, cols = w_out.shape
        chips = n_tp // 2
        hops = n // 2
        piece_cols = width // QUARTERS
        quarter = HEAD // 4
        inverse = 10000.0 ** (-np.arange(quarter) * 2.0 / (2 * quarter))
        inverse = jnp.asarray(np.tile(inverse, 4)[None, :].astype(np.float32))
        bf16, f32 = jnp.bfloat16, jnp.float32
        dma = pltpu.SemaphoreType.DMA
        return pl.pallas_call(
            functools.partial(fused, (n, n_tp)),
            out_shape=jax.ShapeDtypeStruct((own_rows, width), bf16),
            in_specs=[pl.BlockSpec(memory_space=pltpu.HBM)] * 9,
            out_specs=pl.BlockSpec(memory_space=pltpu.HBM),
            scratch_shapes=[
                pltpu.VMEM((own_rows, width), bf16),
                pltpu.VMEM((own_rows, width), bf16),
                pltpu.VMEM((1, width), f32),
                pltpu.VMEM((1, HEAD), f32),
                pltpu.VMEM((1, HEAD), f32),
                pltpu.VMEM((1, HEAD), f32),
                pltpu.VMEM((n_tp, own_rows, width), bf16),
                pltpu.VMEM((n, depth, 2 * HEAD), bf16),
                pltpu.VMEM((n, 2, depth, q_cols), bf16),
                pltpu.VMEM((n, 2, out_rows, cols), bf16),
                pltpu.VMEM((n, 2, rows, HEAD), bf16),
                pltpu.VMEM((rows, HEAD), f32),
                pltpu.VMEM((rows, HEAD), f32),
                pltpu.VMEM((heads, rows, HEAD), bf16),
                pltpu.VMEM((heads, rows, HEAD), f32),
                pltpu.VMEM((heads, rows, HEAD), f32),
                pltpu.VMEM((heads, rows, HEAD), f32),
                pltpu.VMEM((QUARTERS, 2, chips, own_rows, piece_cols), bf16),
                pltpu.VMEM((QUARTERS, chips, own_rows, piece_cols), bf16),
                pltpu.VMEM((QUARTERS, 2, 3, own_rows // 2, piece_cols), bf16),
                pltpu.VMEM((QUARTERS, 2, own_rows // 2, piece_cols), bf16),
                pltpu.VMEM((QUARTERS, 2, own_rows, piece_cols), bf16),
                dma((9,)),
                dma((QUARTERS,)),
                pltpu.SemaphoreType.REGULAR,
                dma((chips - 1,)),
                dma((chips - 1,)),
                dma((chips,)),
                dma((chips,)),
                dma((2,)),
                dma((2, hops // FAR, FAR)),
                dma((2,)),
                dma((2, 2, hops // MID, MID)),
                dma((3,)),
                dma((3,)),
                dma((2,)),
                dma((2,)),
                dma((2,)),
                dma((2, hops, CHUNKS)),
                dma((1,)),
                dma((2, hops + 1)),
                dma((QUARTERS,)),
                dma((QUARTERS,)),
                dma((QUARTERS, 2, 3)),
                dma((QUARTERS, 2, 3)),
            ],
            compiler_params=pltpu.CompilerParams(
                collective_id=0, has_side_effects=True, vmem_limit_bytes=56 * 1024 * 1024
            ),
        )(
            tokens,
            input_gain[None, :],
            w_query,
            w_key,
            w_value,
            query_gain[None, :],
            key_gain[None, :],
            w_out,
            inverse,
        )

    in_specs = (
        P(("grp", "sp", "tp"), None),
        P(),
        P("sp", "tp"),
        P("sp", None),
        P("sp", None),
        P(),
        P(),
        P("tp", "sp"),
    )
    out_specs = P(("grp", "sp", "tp"), None)
    return jax.shard_map(local, mesh=mesh, in_specs=in_specs, out_specs=out_specs, check_vma=False)
```

```python
import functools

import jax
import jax.numpy as jnp
import numpy as np
from jax import lax
from jax.experimental import pallas as pl
from jax.experimental.pallas import tpu as pltpu
from jax.sharding import PartitionSpec as P

HEAD = 128
GRID_W = 64
EPS = 1e-06
CHUNKS = 4
FAR = 4
MID = (2, 2)
LEAD = 8
ALONE = 4
QUARTERS = 4
MESH = pl.DeviceIdType.MESH


def remote(src, dst, send_sem, recv_sem, device):
    return pltpu.make_async_remote_copy(
        src_ref=src, dst_ref=dst, send_sem=send_sem, recv_sem=recv_sem, device_id=device, device_id_type=MESH
    )


def fused(
    sizes,
    tok_hbm,
    gain_hbm,
    wq_hbm,
    wk_hbm,
    wv_hbm,
    qg_hbm,
    kg_hbm,
    wo_hbm,
    inv_hbm,
    out_hbm,
    mixed,
    tok,
    gain,
    qg,
    kg,
    inv,
    normed,
    wkv,
    wq,
    wo,
    kv,
    cosine,
    sine,
    queries,
    peak,
    total,
    summed,
    terms,
    partner_terms,
    pair_sums,
    relayed,
    arrived,
    in_sems,
    out_sems,
    nx_ss,
    nx_rs,
    nd_ss,
    nd_rs,
    wkv_ss,
    wkv_rs,
    w_ss,
    w_rs,
    twin_ss,
    twin_rs,
    md_ss,
    md_rs,
    kv_ss,
    kv_rs,
    kd_ss,
    kd_rs,
    td_ss,
    td_rs,
    x_ss,
    x_rs,
):
    n, n_tp = sizes
    chips = n_tp // 2
    hops = n // 2
    grp, z, t = lax.axis_index("grp"), lax.axis_index("sp"), lax.axis_index("tp")
    x, core = t // 2, t % 2
    half = grp % 2
    other_t = t + 1 - 2 * core
    low_t = t - core
    mate = {"tp": other_t}
    other_grp = grp + 1 - 2 * half
    across = [{"tp": lax.rem(t + 2 * d, n_tp)} for d in range(1, chips)]

    own_rows, width = tok.shape
    rows = own_rows * n_tp
    q_cols = wq.shape[3]
    heads = q_cols // HEAD
    cols = wo.shape[3]

    def back(s):
        return lax.rem(z - s + n, n)

    def ahead(s):
        return lax.rem(z + s, n)

    def toward(way, j):
        return ahead(j) if way == 0 else back(j)

    def source(way, d):
        return back(d) if way == 0 else ahead(d)

    columns = pl.ds(pl.multiple_of(x * HEAD, HEAD), HEAD)
    loads = [
        pltpu.make_async_copy(source_ref, target, in_sems.at[i])
        for i, (source_ref, target) in enumerate(
            (
                (wk_hbm.at[:, columns], wkv.at[z, :, pl.ds(0, HEAD)]),
                (wv_hbm.at[:, columns], wkv.at[z, :, pl.ds(HEAD, HEAD)]),
                (tok_hbm, tok),
                (gain_hbm, gain),
                (wq_hbm, wq.at[z, core]),
                (wo_hbm, wo.at[z, core]),
                (qg_hbm, qg),
                (kg_hbm, kg),
                (inv_hbm, inv),
            )
        )
    ]
    for load in loads:
        load.start()

    peers = [mate, {"grp": other_grp}, {"grp": other_grp, "tp": other_t}] + across
    peers += [{"sp": toward(way, j)} for way in (0, 1) for j in range(1, FAR + 1)]
    peers += [{"sp": toward(way, j), "tp": other_t} for way in (0, 1) for j in range(1, max(MID) + 1)]
    barrier = pltpu.get_barrier_semaphore()
    for peer in peers:
        pl.semaphore_signal(barrier, inc=1, device_id=peer, device_id_type=MESH)
    pl.semaphore_wait(barrier, len(peers))

    wkv_half = wkv.shape[1] // 2

    def wkv_piece(slot):
        return wkv.at[slot, pl.ds(pl.multiple_of(half * wkv_half, wkv_half), wkv_half), :]

    def wkv_ring(way, d, j):
        piece = wkv_piece(source(way, d))
        return remote(piece, piece, wkv_ss.at[way], wkv_rs.at[way, d // FAR, j - 1], {"sp": toward(way, j)})

    def wkv_arrival(way, d):
        piece = wkv_piece(source(way, d))
        return remote(
            piece, piece, wkv_ss.at[way], wkv_rs.at[way, (d - 1) // FAR, (d - 1) % FAR], {"sp": toward(way, 1)}
        )

    def wkv_twin(way, d):
        piece = wkv_piece(source(way, d))
        return remote(piece, piece, twin_ss.at[2], twin_rs.at[2], {"grp": other_grp})

    reach = (hops, hops - 1)

    def wkv_send(way, d):
        for j in [FAR] + list(range(1, FAR)):
            if d + j <= reach[way]:
                wkv_ring(way, d, j).start()

    weights = (wq, wo)

    def half_rows(f):
        size = weights[f].shape[2] // 2
        return pl.ds(pl.multiple_of(half * size, size), size)

    def w_piece(f, slot):
        return weights[f].at[slot, :, half_rows(f), :]

    def w_own(f, way, j):
        piece = weights[f].at[z, core, half_rows(f), :]
        return remote(piece, piece, w_ss.at[f], w_rs.at[f, way, 0, j - 1], {"sp": toward(way, j), "tp": low_t})

    def w_ring(f, way, k, j):
        piece = w_piece(f, source(way, MID[f] * k))
        return remote(piece, piece, w_ss.at[f], w_rs.at[f, way, k, j - 1], {"sp": toward(way, j)})

    def w_arrival(f, way, k, j):
        piece = w_piece(f, source(way, MID[f] * k + j))
        return remote(piece, piece, w_ss.at[f], w_rs.at[f, way, k, j - 1], {"sp": toward(way, 1)})

    def w_share(f, way, d):
        slot = source(way, d)
        for c in (0, 1):
            piece = weights[f].at[slot, c, half_rows(f), :]
            remote(piece, piece, twin_ss.at[f], twin_rs.at[f], {"grp": other_grp, "tp": low_t + c}).start()
        piece = weights[f].at[slot, 1, half_rows(f), :]
        remote(piece, piece, md_ss.at[f], md_rs.at[f], mate).start()

    def several(f, count, c=None):
        size = weights[f].shape[2] // 2
        if c is None:
            return weights[f].at[pl.ds(0, count), :, pl.ds(0, size), :]
        return weights[f].at[pl.ds(0, count), c, pl.ds(0, size), :]

    chunk = 2 * rows // CHUNKS

    def kv_piece(slot, c):
        return kv.at[slot, c * chunk // rows, pl.ds(c * chunk % rows, chunk), :]

    def kv_ring(way, slot, s, c):
        piece = kv_piece(slot, c)
        return remote(piece, piece, kv_ss.at[way], kv_rs.at[way, s, c], {"sp": toward(way, 1)})

    def kv_mate(way, slot, s, c):
        piece = kv_piece(slot, c)
        return remote(piece, piece, kd_ss.at[0], kd_rs.at[way, s], mate)

    def kv_from_mate(way, slot, s):
        return remote(kv.at[slot], kv.at[slot], kd_ss.at[0], kd_rs.at[way, s], mate)

    def normed_to(d):
        return remote(normed.at[t], normed.at[t], nx_ss.at[d - 1], nx_rs.at[d - 1], across[d - 1])

    def normed_slot(d, of):
        return normed.at[lax.rem(of + n_tp - 2 * d, n_tp)]

    def normed_mate(d):
        return remote(normed_slot(d, t), normed_slot(d, t), nd_ss.at[d], nd_rs.at[d], mate)

    def normed_from(d):
        return remote(normed_slot(d, t), normed_slot(d, t), nx_ss.at[d - 1], nx_rs.at[d - 1], across[d - 1])

    def normed_from_mate(d):
        return remote(normed_slot(d, other_t), normed_slot(d, other_t), nd_ss.at[d], nd_rs.at[d], mate)

    loads[0].wait()
    loads[1].wait()

    @pl.when(core == 1)
    def _():
        wkv_send(0, 0)
        wkv_send(1, 0)

    loads[2].wait()
    loads[3].wait()
    floats = tok[...].astype(jnp.float32)
    scale = lax.rsqrt(jnp.mean(floats * floats, axis=-1, keepdims=True) + EPS)
    normed[t] = (floats * scale * gain[...]).astype(jnp.bfloat16)
    for d in range(1, chips):
        normed_to(d).start()
    normed_mate(0).start()

    def w_own_sends(f):
        loads[4 + f].wait()
        for j in range(MID[f], 0, -1):
            for way in (0, 1):
                w_own(f, way, j).start()

    for load in loads[6:]:
        load.wait()

    lane = lax.broadcasted_iota(jnp.int32, (rows, HEAD), 1)
    place = lax.broadcasted_iota(jnp.int32, (rows, HEAD), 0) + z * rows
    spot = jnp.where(lane < HEAD // 2, place // GRID_W, place % GRID_W).astype(jnp.float32)
    angles = spot * inv[...]
    first_half = lane % (HEAD // 2) < HEAD // 4
    cosine[...] = jnp.cos(angles)
    sine[...] = jnp.where(first_half, -jnp.sin(angles), jnp.sin(angles))
    peak[...] = jnp.full_like(peak, -1e30)
    total[...] = jnp.zeros_like(total)
    summed[...] = jnp.zeros_like(summed)

    def turned(raw, head_gain):
        heads_in = raw.astype(jnp.bfloat16).astype(jnp.float32)
        scale = lax.rsqrt(jnp.mean(heads_in * heads_in, axis=-1, keepdims=True) + EPS)
        scaled = heads_in * scale * head_gain
        lanes = lax.broadcasted_iota(jnp.int32, scaled.shape, 1)
        other = jnp.where(
            lanes % (HEAD // 2) < HEAD // 4,
            pltpu.roll(scaled, HEAD - HEAD // 4, 1),
            pltpu.roll(scaled, HEAD // 4, 1),
        )
        return scaled * cosine[...] + other * sine[...]

    def query_weights_here():
        incoming = several(0, n - 1, 0)
        remote(incoming, incoming, twin_ss.at[0], twin_rs.at[0], mate).wait_recv()

    def make_queries(first, count):
        raw = jnp.dot(
            normed[...].reshape(rows, width),
            wq[:, core, :, first * HEAD : (first + count) * HEAD].reshape(width, count * HEAD),
            preferred_element_type=jnp.float32,
        )
        for h in range(count):
            queries[first + h] = (turned(raw[:, h * HEAD : (h + 1) * HEAD], qg[...]) * HEAD ** (-0.5)).astype(
                jnp.bfloat16
            )

    def attend(a, b):
        pieces = [(h, pl.ds(r, HEAD)) for h in range(heads) for r in range(0, rows, HEAD)]
        scores = [
            [
                lax.dot_general(
                    queries[h, part], kv[i, 0], (((1,), (1,)), ((), ())), preferred_element_type=jnp.float32
                )
                for i in (a, b)
            ]
            for h, part in pieces
        ]
        peaks = []
        for (h, part), pair in zip(pieces, scores):
            highest = jnp.maximum(*pair)
            highest = functools.reduce(
                jnp.maximum, [highest[:, i : i + HEAD] for i in range(0, rows, HEAD)]
            )
            peaks.append(jnp.maximum(peak[h, part], jnp.max(highest, axis=1, keepdims=True)))
        for (h, part), pair, new in zip(pieces, scores, peaks):
            fade = jnp.exp(peak[h, part] - new)
            wide = jnp.concatenate([new] * (rows // HEAD), axis=1)
            parts = [jnp.exp(score - wide) for score in pair]
            peak[h, part] = new
            added = parts[0] + parts[1]
            total[h, part] = fade * total[h, part] + sum(added[:, i : i + HEAD] for i in range(0, rows, HEAD))
            summed[h, part] = (
                fade * summed[h, part]
                + jnp.dot(parts[0].astype(jnp.bfloat16), kv[a, 1], preferred_element_type=jnp.float32)
                + jnp.dot(parts[1].astype(jnp.bfloat16), kv[b, 1], preferred_element_type=jnp.float32)
            )

    @pl.when(core == 1)
    def _():
        w_own_sends(0)
        for k in range(1, hops // FAR + 1):
            for way in (0, 1):
                if FAR * k <= reach[way]:
                    wkv_arrival(way, FAR * k).wait_recv()
                    wkv_send(way, FAR * k)
                    wkv_twin(way, FAR * k).start()
            for d in range(FAR * (k - 1) + 1, FAR * k):
                for way in (0, 1):
                    wkv_arrival(way, d).wait_recv()
                    wkv_twin(way, d).start()
        w_own_sends(1)
        for d in range(1, chips):
            normed_from(d).wait_recv()
        for d in range(chips):
            normed_from_mate(d).wait_recv()
        incoming = wkv.at[pl.ds(0, n - 1), pl.ds(0, wkv_half), :]
        remote(incoming, incoming, twin_ss.at[2], twin_rs.at[2], mate).wait_recv()
        projected = jnp.dot(
            normed[...].reshape(rows, width),
            wkv[...].reshape(width, 2 * HEAD),
            preferred_element_type=jnp.float32,
        )
        kv[z, 0] = turned(projected[:, :HEAD], kg[...]).astype(jnp.bfloat16)
        kv[z, 1] = projected[:, HEAD:].astype(jnp.bfloat16)
        for c in range(CHUNKS):
            kv_ring(0, z, 0, c).start()
            kv_ring(1, z, 0, c).start()
        for c in range(CHUNKS):
            kv_mate(0, z, 0, c).start()
        for d in range(1, chips):
            normed_mate(d).start()

        def kv_step(s):
            for c in range(CHUNKS):
                kv_ring(0, back(s), s - 1, c).wait_recv()
                kv_ring(0, back(s), s, c).start()
                kv_mate(0, back(s), s, c).start()
                kv_ring(1, ahead(s), s - 1, c).wait_recv()

                @pl.when(s < hops - 1)
                def _():
                    kv_ring(1, ahead(s), s, c).start()

                kv_mate(1, ahead(s), s, c).start()

        def early(s, carry):
            kv_step(s)
            return carry

        lax.fori_loop(1, LEAD + 1, early, 0)
        for h in range(heads):
            kv_step(LEAD + 1 + h)
            if h == 0:
                incoming = several(0, n - 1, 0)
                remote(incoming, incoming, md_ss.at[0], md_rs.at[0], mate).wait_recv()
                query_weights_here()
            make_queries(h, 1)
        lead = LEAD + heads
        pace = -(-(hops - 1) // (hops - 1 - lead))

        def pair(i, carry):
            attend(back(i), ahead(i))
            return carry

        def late(s, carry):
            kv_step(s)
            first = jnp.minimum(pace * (s - 1 - lead), s - 1) + 1
            lax.fori_loop(first, jnp.minimum(pace * (s - lead), s) + 1, pair, 0)
            return carry

        lax.fori_loop(lead + 1, hops, late, 0)
        for c in range(CHUNKS):
            kv_ring(0, back(hops), hops - 1, c).wait_recv()
            kv_mate(0, back(hops), hops, c).start()
        attend(z, back(hops))
        incoming = several(1, n - 1, 0)
        remote(incoming, incoming, md_ss.at[1], md_rs.at[1], mate).wait_recv()

    @pl.when(core == 0)
    def _():
        def w_step(f, k):
            mid = MID[f]
            w_arrival(f, 0, k - 1, mid).wait_recv()
            for j in range(mid, 0, -1):
                w_ring(f, 0, k, j).start()
            w_share(f, 0, mid * k)
            w_arrival(f, 1, k - 1, mid).wait_recv()
            if mid == 1:
                pl.when(k + 1 < hops)(lambda: w_ring(f, 1, k, 1).start())
            else:
                pl.when(mid * (k + 1) < hops)(lambda: w_ring(f, 1, k, mid).start())
                for j in range(mid - 1, 0, -1):
                    w_ring(f, 1, k, j).start()
            w_share(f, 1, mid * k)
            for j in range(1, mid):
                for way in (0, 1):
                    w_arrival(f, way, k - 1, j).wait_recv()
                    w_share(f, way, mid * (k - 1) + j)

        def w_end(f):
            mid = MID[f]
            k = hops // mid
            w_arrival(f, 0, k - 1, mid).wait_recv()
            w_share(f, 0, mid * k)
            for j in range(1, mid):
                for way in (0, 1):
                    w_arrival(f, way, k - 1, j).wait_recv()
                    w_share(f, way, mid * (k - 1) + j)

        def query_step(k, carry):
            w_step(0, k)
            return carry

        def both_step(k, carry):
            w_step(0, k)
            w_step(1, k - ALONE + 1)
            return carry

        q_last, o_last = hops // MID[0], hops // MID[1]
        w_own_sends(0)
        lax.fori_loop(1, min(3, ALONE), query_step, 0)
        for d in range(1, chips):
            normed_from(d).wait_recv()
            normed_mate(d).start()
        lax.fori_loop(min(3, ALONE), ALONE, query_step, 0)
        w_own_sends(1)
        lax.fori_loop(ALONE, q_last, both_step, 0)
        w_end(0)
        for d in range(chips):
            normed_from_mate(d).wait_recv()
        query_weights_here()
        make_queries(0, heads)

        def pair(s, carry):
            kv_from_mate(0, back(s), s).wait_recv()
            kv_from_mate(1, ahead(s), s).wait_recv()
            attend(back(s), ahead(s))
            return carry

        done = q_last - ALONE
        each = -(-(hops - 1) // (o_last - 1 - done)) if o_last - 1 > done else hops

        def out_step(k, carry):
            w_step(1, k)
            i = k - done - 1
            first = jnp.minimum(each * i, hops - 1) + 1
            return lax.fori_loop(first, jnp.minimum(each * (i + 1), hops - 1) + 1, pair, carry)

        lax.fori_loop(done + 1, o_last, out_step, 0)
        w_end(1)
        lax.fori_loop(min(each * max(o_last - 1 - done, 0), hops - 1) + 1, hops, pair, 0)
        kv_from_mate(0, z, 0).wait_recv()
        kv_from_mate(0, back(hops), hops).wait_recv()
        attend(z, back(hops))

    attended = jnp.concatenate(
        [
            (summed[h] / jnp.sum(total[h], axis=1, keepdims=True)).astype(jnp.bfloat16)
            for h in range(heads)
        ],
        axis=1,
    )
    incoming = several(1, n - 1, 0)
    remote(incoming, incoming, twin_ss.at[1], twin_rs.at[1], mate).wait_recv()

    per_piece = n // QUARTERS

    def term_mate(p):
        return remote(terms.at[p, 1 - core], partner_terms.at[p], td_ss.at[p], td_rs.at[p], mate)

    def project(p, carry):
        for j in range(per_piece // 2):
            first = p * per_piece + 2 * j
            both = jnp.concatenate([wo[first, core], wo[first + 1, core]], axis=1)
            term = jnp.dot(attended, both, preferred_element_type=jnp.float32).astype(jnp.bfloat16)
            for owner in range(n_tp):
                terms[p, owner % 2, owner // 2, :, 2 * j * cols : (2 * j + 2) * cols] = term[
                    owner * own_rows : (owner + 1) * own_rows
                ]
        term_mate(p).start()
        return carry

    lax.fori_loop(0, QUARTERS, project, 0)

    near = own_rows // 2
    upper, lower = pl.ds(0, near), pl.ds(near, near)
    ways = ((1, upper, lower), (chips - 1, lower, upper))

    def pair_sum(p, there, part):
        return terms[p, core, there, part].astype(jnp.float32) + partner_terms[p, there, part].astype(jnp.float32)

    def x_send(src, dst, p, way, i):
        return remote(src, dst, x_ss.at[p, way, i], x_rs.at[p, way, i], across[ways[way][0] - 1])

    def far_part(p, way):
        return x_send(pair_sums.at[p, way, 0], relayed.at[p, way], p, way, 0)

    def near_part(p, way):
        return x_send(pair_sums.at[p, way, 1], arrived.at[p, way, ways[way][2]], p, way, 1)

    def passed_part(p, way):
        return x_send(pair_sums.at[p, way, 2], arrived.at[p, way, ways[way][1]], p, way, 2)

    def send_sums(p):
        term_mate(p).wait_recv()
        for way, (on, passed, kept) in enumerate(ways):
            pair_sums[p, way, 0] = pair_sum(p, lax.rem(x + 2, chips), passed).astype(jnp.bfloat16)
            far_part(p, way).start()
        for way, (on, passed, kept) in enumerate(ways):
            pair_sums[p, way, 1] = pair_sum(p, lax.rem(x + on, chips), kept).astype(jnp.bfloat16)
            near_part(p, way).start()

    def pass_on(p):
        for way, (on, passed, kept) in enumerate(ways):
            far_part(p, way).wait_recv()
            both = pair_sum(p, lax.rem(x + on, chips), passed) + relayed[p, way].astype(jnp.float32)
            pair_sums[p, way, 2] = both.astype(jnp.bfloat16)
            passed_part(p, way).start()

    send_sums(0)
    for p in range(1, QUARTERS):
        send_sums(p)
        pass_on(p - 1)
    pass_on(QUARTERS - 1)
    piece_cols = per_piece * cols

    def out_copy(p):
        part = pl.ds(p * piece_cols, piece_cols)
        return pltpu.make_async_copy(mixed.at[:, part], out_hbm.at[:, part], out_sems.at[p])

    for p in range(QUARTERS):
        for way in (0, 1):
            near_part(p, way).wait_recv()
            passed_part(p, way).wait_recv()
        rows_sum = pair_sum(p, x, pl.ds(0, own_rows))
        for way in (0, 1):
            rows_sum = rows_sum + arrived[p, way].astype(jnp.float32)
        mixed[:, p * piece_cols : (p + 1) * piece_cols] = rows_sum.astype(mixed.dtype)
        out_copy(p).start()

    for p in range(QUARTERS):
        out_copy(p).wait()
    for d in range(1, chips):
        normed_to(d).wait_send()
    for d in range(chips):
        normed_mate(d).wait_send()

    @pl.when(core == 1)
    def _():
        for way in (0, 1):
            sends = sum(1 for d in range(0, reach[way], FAR) for j in range(1, FAR + 1) if d + j <= reach[way])
            sent = wkv.at[pl.ds(0, sends), pl.ds(0, wkv_half), :]
            remote(sent, sent, wkv_ss.at[way], wkv_rs.at[way, 0, 0], mate).wait_send()
            sent = kv.at[pl.ds(0, reach[way])]
            remote(sent, sent, kv_ss.at[way], kv_rs.at[way, 0, 0], mate).wait_send()
        sent = wkv.at[pl.ds(0, n - 1), pl.ds(0, wkv_half), :]
        remote(sent, sent, twin_ss.at[2], twin_rs.at[2], mate).wait_send()
        remote(kv, kv, kd_ss.at[0], kd_rs.at[0, 0], mate).wait_send()
        for f in (0, 1):
            sent = several(f, 2 * MID[f], 0)
            remote(sent, sent, w_ss.at[f], w_rs.at[f, 0, 0, 0], mate).wait_send()

    @pl.when(core == 0)
    def _():
        for f in (0, 1):
            sent = several(f, n - 1 - MID[f])
            remote(sent, sent, w_ss.at[f], w_rs.at[f, 0, 0, 0], mate).wait_send()
            sent = several(f, n - 1)
            remote(sent, sent, twin_ss.at[f], twin_rs.at[f], mate).wait_send()
            sent = several(f, n - 1, 0)
            remote(sent, sent, md_ss.at[f], md_rs.at[f], mate).wait_send()

    for p in range(QUARTERS):
        term_mate(p).wait_send()
        for way in (0, 1):
            far_part(p, way).wait_send()
            near_part(p, way).wait_send()
            passed_part(p, way).wait_send()


def solution(mesh):
    n, n_tp = mesh.shape["sp"], mesh.shape["tp"]

    def local(tokens, input_gain, w_query, w_key, w_value, query_gain, key_gain, w_out):
        own_rows, width = tokens.shape
        rows = own_rows * n_tp
        depth, q_cols = w_query.shape
        heads = q_cols // HEAD
        out_rows, cols = w_out.shape
        chips = n_tp // 2
        hops = n // 2
        piece_cols = width // QUARTERS
        quarter = HEAD // 4
        inverse = 10000.0 ** (-np.arange(quarter) * 2.0 / (2 * quarter))
        inverse = jnp.asarray(np.tile(inverse, 4)[None, :].astype(np.float32))
        bf16, f32 = jnp.bfloat16, jnp.float32
        dma = pltpu.SemaphoreType.DMA
        return pl.pallas_call(
            functools.partial(fused, (n, n_tp)),
            out_shape=jax.ShapeDtypeStruct((own_rows, width), bf16),
            in_specs=[pl.BlockSpec(memory_space=pltpu.HBM)] * 9,
            out_specs=pl.BlockSpec(memory_space=pltpu.HBM),
            scratch_shapes=[
                pltpu.VMEM((own_rows, width), bf16),
                pltpu.VMEM((own_rows, width), bf16),
                pltpu.VMEM((1, width), f32),
                pltpu.VMEM((1, HEAD), f32),
                pltpu.VMEM((1, HEAD), f32),
                pltpu.VMEM((1, HEAD), f32),
                pltpu.VMEM((n_tp, own_rows, width), bf16),
                pltpu.VMEM((n, depth, 2 * HEAD), bf16),
                pltpu.VMEM((n, 2, depth, q_cols), bf16),
                pltpu.VMEM((n, 2, out_rows, cols), bf16),
                pltpu.VMEM((n, 2, rows, HEAD), bf16),
                pltpu.VMEM((rows, HEAD), f32),
                pltpu.VMEM((rows, HEAD), f32),
                pltpu.VMEM((heads, rows, HEAD), bf16),
                pltpu.VMEM((heads, rows, HEAD), f32),
                pltpu.VMEM((heads, rows, HEAD), f32),
                pltpu.VMEM((heads, rows, HEAD), f32),
                pltpu.VMEM((QUARTERS, 2, chips, own_rows, piece_cols), bf16),
                pltpu.VMEM((QUARTERS, chips, own_rows, piece_cols), bf16),
                pltpu.VMEM((QUARTERS, 2, 3, own_rows // 2, piece_cols), bf16),
                pltpu.VMEM((QUARTERS, 2, own_rows // 2, piece_cols), bf16),
                pltpu.VMEM((QUARTERS, 2, own_rows, piece_cols), bf16),
                dma((9,)),
                dma((QUARTERS,)),
                dma((chips - 1,)),
                dma((chips - 1,)),
                dma((chips,)),
                dma((chips,)),
                dma((2,)),
                dma((2, hops // FAR, FAR)),
                dma((2,)),
                dma((2, 2, hops // min(MID), max(MID))),
                dma((3,)),
                dma((3,)),
                dma((2,)),
                dma((2,)),
                dma((2,)),
                dma((2, hops, CHUNKS)),
                dma((1,)),
                dma((2, hops + 1)),
                dma((QUARTERS,)),
                dma((QUARTERS,)),
                dma((QUARTERS, 2, 3)),
                dma((QUARTERS, 2, 3)),
            ],
            compiler_params=pltpu.CompilerParams(
                collective_id=0, has_side_effects=True, vmem_limit_bytes=56 * 1024 * 1024
            ),
        )(
            tokens,
            input_gain[None, :],
            w_query,
            w_key,
            w_value,
            query_gain[None, :],
            key_gain[None, :],
            w_out,
            inverse,
        )

    in_specs = (
        P(("grp", "sp", "tp"), None),
        P(),
        P("sp", "tp"),
        P("sp", None),
        P("sp", None),
        P(),
        P(),
        P("tp", "sp"),
    )
    out_specs = P(("grp", "sp", "tp"), None)
    return jax.shard_map(local, mesh=mesh, in_specs=in_specs, out_specs=out_specs, check_vma=False)
```
